256 devices in a mesh: grp: 2 (over y), fs: 32 (over z, core), tp: 4 (over x).
Axes of the slice: x: 4, y: 2, z: 16, core: 2. Of those that a mesh axis runs over, the one named last changes fastest.
The devices are a block of a 4x16x16 slice.
Arguments:
- tokens: bfloat16 [14336, 2048], P(('grp', 'fs'), 'tp'), parts along dimension 0, may hold values from -170 to 170
- routes: int32 [14336, 6], P(('grp', 'fs')), parts along dimension 0, may hold values from 0 to 63, all different within a row; in each aligned block of 224 rows (0 to 223, 224 to 447, ...) at most 28 rows name the same one
- route_weights: float32 [14336, 6], P(('grp', 'fs')), parts along dimension 0, may hold values from 0.2 to 1
- norm_gain: float32 [2048], P('fs'), may hold values from 0.1 to 1.9
- gate_experts: float32 [64, 2048, 512], P(None, 'fs', 'tp'), may hold values from -0.125 to 0.125
- up_experts: float32 [64, 2048, 512], P(None, 'fs', 'tp'), may hold values from -0.125 to 0.125
- down_experts: float32 [64, 512, 2048], P(None, 'fs', 'tp'), may hold values from -0.25 to 0.25
- shared_gate: float32 [2048, 512], P('fs', 'tp'), may hold values from -0.125 to 0.125
- shared_up: float32 [2048, 512], P('fs', 'tp'), may hold values from -0.125 to 0.125
- shared_down: float32 [512, 2048], P('fs', 'tp'), may hold values from -0.25 to 0.25
Outputs:
- mixed: bfloat16 [14336, 2048], P(('grp', 'fs'), 'tp'), parts along dimension 0
- gate_ready: bfloat16 [128, 2048, 512], P(('grp', 'fs'), None, 'tp'), parts along dimension 0
- up_ready: bfloat16 [128, 2048, 512], P(('grp', 'fs'), None, 'tp'), parts along dimension 0
- down_ready: bfloat16 [128, 512, 2048], P(('grp', 'fs'), 'tp'), parts along dimension 0
- shared_gate_ready: bfloat16 [4096, 512], P('grp', 'tp'), parts along dimension 0
- shared_up_ready: bfloat16 [4096, 512], P('grp', 'tp'), parts along dimension 0
- shared_down_ready: bfloat16 [1024, 2048], P(('grp', 'tp')), parts along dimension 0
The draws below stay inside these ranges and needn't reach their ends.
There are 2 independent parts, one for each index of `grp`. The reference program is written for one: setup_inputs(seed, part) draws one part's arguments, and reference() takes and returns one part's arrays. A program takes and returns all parts, laid end to end along the dimension named above; an argument that names none is the same for every part. Nothing has to cross between parts.
Inputs may be any that keep to these rules, and one draw needn't show every extreme that they name: `routes`: the 6 experts of a row differ; among the rows of one index of fs no expert is named more than 28 times, a bound that some block reaches.
All inputs are finite; a program needn't handle non-finite values.
Results may differ from the reference program's by a relative error of at most 0.013.
Values may be sent and summed in bfloat16 or wider, within the bound.
No kernel may reach another device: no remote copies, remote signals or barrier semaphores. Data moves between devices by JAX's collectives and lax.ppermute only.
A program may use at most 128 MiB of HBM per device.

```python
import math
import jax
import jax.numpy as jnp
import numpy as np
from jax import lax

D = 2048
FF = 512
SF = 512
EXPERTS = 64
TOP_K = 6
TOK_DEV = 224
TOKENS = 7168
CAP = 28
N_TP = 4


def draw_tokens(key, part):
    key_rows = jax.random.fold_in(key, 11)
    key_cols = jax.random.fold_in(key, 12)
    key_base = jax.random.fold_in(key, 13)
    row_scale = jnp.exp(jax.random.uniform(key_rows, (TOKENS, 1), jnp.float32, 0.0, math.log(10.0)))
    col_scale = jnp.exp(jax.random.uniform(key_cols, (1, D), jnp.float32, 0.0, math.log(10.0)))
    base = jnp.clip(jax.random.normal(key_base, (TOKENS, D), jnp.float32), -5.0, 5.0)
    return (base * row_scale * col_scale / 3.0).astype(jnp.bfloat16)


def block_scale(own_key, dims, cuts, low, top_value):
    def one(dim, blocks):
        steps = jax.random.uniform(jax.random.fold_in(jax.random.fold_in(own_key, 6), dim), (blocks,), jnp.float32, low / len(cuts), top_value / len(cuts))
        return jnp.repeat(jnp.exp(steps), dims[dim] // blocks).reshape((-1,) + (1,) * (len(dims) - dim - 1))

    gain = one(*cuts[0])
    for cut in cuts[1:]:
        gain = gain * one(*cut)
    return gain


def shared_out(rng, own, number, rows, amount, top, most, slope):
    order = jax.random.permutation(rng, amount)
    heavy_load, common = portions_of(amount, rows * top, most, slope, True), portions_of(amount, rows * top, most, slope, False)
    places = jnp.arange(amount)

    def named(lengths, turn):
        used = int((lengths > 0).sum())
        fixed = max(1, used // 4)
        passed = fixed + (places - fixed + turn * (used - fixed)) % max(1, amount - fixed)
        return jnp.zeros((amount,), jnp.int32).at[order[jnp.where(places < fixed, places, passed)]].set(jnp.asarray(lengths, jnp.int32))

    lengths = jnp.where(number % 4 == 0, named(heavy_load, number // 4), named(common, number - number // 4 - 1))
    mixed = jax.random.permutation(jax.random.fold_in(own, 3), amount)
    giver, receiver = mixed[0:amount // 2 * 2:2], mixed[1:amount // 2 * 2:2]
    room = jnp.minimum(lengths[giver] - 1, most - lengths[receiver]) // 2
    room = jnp.where((giver == order[0]) | (receiver == order[0]) | (lengths[receiver] == 0), 0, jnp.maximum(room, 0))
    passed = jax.random.randint(jax.random.fold_in(own, 4), (amount // 2,), 0, 1 << 20) % (room + 1)
    lengths = lengths.at[giver].add(-passed).at[receiver].add(passed)
    members = jnp.searchsorted(jnp.cumsum(lengths), jnp.arange(rows * top), side="right").astype(jnp.int32)
    grid = members.reshape(top, rows).T
    grid = grid[jax.random.permutation(jax.random.fold_in(own, 1), rows)]
    turn = jax.random.randint(jax.random.fold_in(own, 2), (rows, 1), 0, top)
    return jnp.take_along_axis(grid, (jnp.arange(top)[None, :] + turn) % top, axis=1)


def portions_of(amount, total, reach, skew, full):
    portions = [(1 << 20) // math.isqrt(rank ** skew) + 1 for rank in range(1, amount + 1)]
    largest = reach if full else min(reach, max(-(-total // amount), total * portions[0] // sum(portions)))
    least = 1 if total - largest >= amount - 1 else 0
    counts, spare = [largest] + [least] * (amount - 1), total - largest - least * (amount - 1)
    while spare > 0:
        movable = [i for i in range(1, amount) if counts[i] < largest] or [i for i in range(1, amount) if counts[i] < reach]
        pool, left = sum([portions[i] for i in movable]), spare
        for i in movable:
            addition = min(reach - counts[i], max(1, left * portions[i] // pool), spare)
            counts[i] = counts[i] + addition
            spare = spare - addition
    return np.array(counts)


def normal_values(stream_key, shape, scale, most, pieces=(), kind=jnp.bfloat16):
    factor_of = block_scale(stream_key, shape, pieces, -0.22, 0.18) if pieces else 1.0
    array = jax.random.normal(stream_key, shape, jnp.float32) * scale * factor_of
    return jnp.minimum(jnp.maximum(array, -most), most).astype(kind)


def setup_inputs(seed: int = 0, part: int = 0) -> dict:
    splits = jax.random.split(jax.random.key(seed), 11)
    part_splits = jax.random.split(jax.random.fold_in(splits[10], part), 11)
    tokens = draw_tokens(jax.random.fold_in(jax.random.fold_in(splits[10], part), 71), part)
    routes_keys = jax.random.split(jax.random.fold_in(part_splits[1], 1), TOKENS // TOK_DEV)
    routes_turns = jax.random.permutation(jax.random.fold_in(part_splits[1], 3), TOKENS // TOK_DEV)
    routes = jax.vmap(lambda own, number: shared_out(jax.random.fold_in(part_splits[1], 2), own, number, TOK_DEV, EXPERTS, TOP_K, CAP, 1))(routes_keys, routes_turns).reshape((TOKENS, TOP_K))
    route_weights = jnp.clip(jnp.exp(math.log(1.0) - 1.609438 * jax.random.uniform(part_splits[2], (TOKENS, TOP_K), jnp.float32) ** block_scale(part_splits[2], (TOKENS, TOP_K), ((0, 32),), -0.2, 0.2)), 0.2, 1.0)
    norm_gain = jnp.clip(1.0 + 0.18 * jax.random.normal(splits[3], (D,), jnp.float32), 0.1, 1.9)
    gate_experts = normal_values(splits[4], (EXPERTS, D, FF), D ** -0.5, 0.125, ((1, 32), (2, 4)), jnp.float32)
    up_experts = normal_values(splits[5], (EXPERTS, D, FF), D ** -0.5, 0.125, ((1, 32), (2, 4)), jnp.float32)
    down_experts = normal_values(splits[6], (EXPERTS, FF, D), FF ** -0.5, 0.25, ((1, 32), (2, 4)), jnp.float32)
    shared_gate = normal_values(splits[7], (D, SF), D ** -0.5, 0.125, ((0, 32), (1, 4)), jnp.float32)
    shared_up = normal_values(splits[8], (D, SF), D ** -0.5, 0.125, ((0, 32), (1, 4)), jnp.float32)
    shared_down = normal_values(splits[9], (SF, D), SF ** -0.5, 0.25, ((0, 32), (1, 4)), jnp.float32)
    return {"tokens": tokens, "routes": routes, "route_weights": route_weights, "norm_gain": norm_gain, "gate_experts": gate_experts, "up_experts": up_experts, "down_experts": down_experts, "shared_gate": shared_gate, "shared_up": shared_up, "shared_down": shared_down}


def grouped_product(active, weight):
    groups = N_TP
    span_cols = active.shape[1] // groups
    totals = jnp.zeros((active.shape[0], weight.shape[1]), jnp.float32)
    for section in range(groups):
        product = jnp.dot(active[:, section * span_cols:(section + 1) * span_cols], weight[section * span_cols:(section + 1) * span_cols], preferred_element_type=jnp.float32)
        rounded = lax.optimization_barrier(product.astype(jnp.bfloat16))
        totals = totals + rounded.astype(jnp.float32)
    return totals

def reference(tokens, routes, route_weights, norm_gain, gate_experts, up_experts, down_experts, shared_gate, shared_up, shared_down):
    gate_ready = (gate_experts * norm_gain[None, :, None]).astype(jnp.bfloat16)
    up_ready = (up_experts * norm_gain[None, :, None]).astype(jnp.bfloat16)
    down_ready = down_experts.astype(jnp.bfloat16)
    shared_gate_ready = (shared_gate * norm_gain[:, None]).astype(jnp.bfloat16)
    shared_up_ready = (shared_up * norm_gain[:, None]).astype(jnp.bfloat16)
    shared_down_ready = shared_down.astype(jnp.bfloat16)
    widened = tokens.astype(jnp.float32)
    normed = (widened * lax.rsqrt(lax.optimization_barrier(jnp.mean(widened * widened, axis=1, keepdims=True)) + 1e-06)).astype(jnp.bfloat16)
    shared_active = (jax.nn.silu(jnp.dot(normed, shared_gate_ready, preferred_element_type=jnp.float32)) * jnp.dot(normed, shared_up_ready, preferred_element_type=jnp.float32)).astype(jnp.bfloat16)
    shared_rows = grouped_product(shared_active, shared_down_ready)
    blocks = TOKENS // TOK_DEV
    pairs = TOK_DEV * TOP_K
    block_routes = routes.reshape(blocks, pairs)
    onehot = (block_routes[:, :, None] == jnp.arange(EXPERTS, dtype=jnp.int32)[None, None, :]).astype(jnp.int32)
    earlier = jnp.cumsum(onehot, axis=1) - onehot
    slot_index = lax.optimization_barrier(jnp.sum(earlier * onehot, axis=2)).astype(jnp.int32)
    target = block_routes * CAP + slot_index
    token_index = (jnp.arange(TOKENS * TOP_K, dtype=jnp.int32) // TOP_K).astype(jnp.int32)
    flat_target = (target + (jnp.arange(blocks, dtype=jnp.int32) * (EXPERTS * CAP))[:, None]).reshape(-1)
    source = jnp.full((blocks * EXPERTS * CAP,), -1, jnp.int32).at[flat_target].set(token_index)
    source = source.reshape(blocks, EXPERTS, CAP).transpose(1, 0, 2).reshape(EXPERTS, blocks * CAP)

    def expert_rows(operands):
        row_index, gate_one, up_one, down_one = operands
        present = row_index >= 0
        inputs = jnp.where(present[:, None], normed[jnp.maximum(row_index, 0)], jnp.zeros((), jnp.bfloat16))
        active = (jax.nn.silu(jnp.dot(inputs, gate_one, preferred_element_type=jnp.float32)) * jnp.dot(inputs, up_one, preferred_element_type=jnp.float32)).astype(jnp.bfloat16)
        return grouped_product(active, down_one).astype(jnp.bfloat16)
    results = lax.map(expert_rows, (source, gate_ready, up_ready, down_ready))
    flat_results = results.reshape(EXPERTS * blocks * CAP, D)
    block_of = (jnp.arange(TOKENS, dtype=jnp.int32) // TOK_DEV)[:, None]
    position = routes * (blocks * CAP) + block_of * CAP + slot_index.reshape(TOKENS, TOP_K)
    mixed = shared_rows
    for choice_k in range(TOP_K):
        mixed = mixed + flat_results[position[:, choice_k]].astype(jnp.float32) * route_weights[:, choice_k:choice_k + 1]
    return (mixed.astype(jnp.bfloat16), gate_ready, up_ready, down_ready, shared_gate_ready, shared_up_ready, shared_down_ready)
```

```python
import functools

import jax
import jax.numpy as jnp
from jax import lax
from jax.experimental import pallas as pl
from jax.experimental.pallas import tpu as pltpu
from jax.sharding import Mesh
from jax.sharding import PartitionSpec as P


BF = jnp.bfloat16
F32 = jnp.float32
LANES = 128
VMEM = pl.BlockSpec(memory_space=pltpu.VMEM)
SMEM = pl.BlockSpec(memory_space=pltpu.SMEM)


def call(body, name, scalars, arrays, outs, flops):
    moved = sum(a.size * a.dtype.itemsize for a in arrays) + sum(
        o.size * o.dtype.itemsize for o in outs
    )
    return pl.pallas_call(
        body,
        name=name,
        out_shape=tuple(outs),
        in_specs=[SMEM] * len(scalars) + [VMEM] * len(arrays),
        out_specs=tuple([VMEM] * len(outs)),
        cost_estimate=pl.CostEstimate(flops=flops, bytes_accessed=moved, transcendentals=0),
    )(*scalars, *arrays)


def shift(x, axis, size, by):
    return lax.ppermute(x, axis, [(i, (i + by) % size) for i in range(size)])


def ring_gather(x, axis, size):
    held = {0: x}
    right = left = x
    for step in range(1, size // 2 + 1):
        right = shift(right, axis, size, 1)
        held[step] = right
        if step < size - step:
            left = shift(left, axis, size, -1)
            held[-step] = left
    return held


def quarters(x, size):
    half = x.shape[0] // 2
    a = shift(x, "tp", size, 1)
    b = shift(x, "tp", size, -1)
    c = shift(a[:half], "tp", size, 1)
    d = shift(b[half:], "tp", size, -1)
    return x, a, b, c, d


def pack_body(tok, routes, weights, sgate, sup, sdown, gain, chunk, meta):
    rows = tok.shape[0]
    top = routes.shape[0]
    experts = 64
    chunk[:rows, :] = tok[...]
    meta[...] = jnp.full(meta.shape, -1.0, F32)
    which = lax.broadcasted_iota(jnp.int32, (experts, rows), 0)
    named = [routes[k : k + 1, :] == which for k in range(top)]
    member = sum(jnp.where(n, 1.0, 0.0) for n in named)
    before = (
        lax.broadcasted_iota(jnp.int32, (rows, rows), 0)
        < lax.broadcasted_iota(jnp.int32, (rows, rows), 1)
    )
    count = jnp.dot(
        member.astype(BF), jnp.where(before, 1.0, 0.0).astype(BF), preferred_element_type=F32
    )
    ids = routes[...].astype(F32)
    spare = rows - LANES
    for k in range(top):
        place = jnp.sum(jnp.where(named[k], count, 0.0), axis=0, keepdims=True)
        meta[16 + k : 17 + k, :] = place[:, :LANES]
        meta[24 + k : 25 + k, :spare] = place[:, LANES:]
    meta[0:top, :] = ids[:, :LANES]
    meta[8 : 8 + top, :spare] = ids[:, LANES:]
    w = weights[...]
    meta[32 : 32 + top, :] = w[:, :LANES]
    meta[40 : 40 + top, :spare] = w[:, LANES:]
    scale = gain[...]
    chunk[rows:, 0:128] = (sgate[...] * scale).astype(BF)
    chunk[rows:, 128:256] = (sup[...] * scale).astype(BF)
    for c in range(4):
        chunk[rows + 16 * c : rows + 16 * c + 16, 256:384] = sdown[
            :, 128 * c : 128 * c + 128
        ].astype(BF)
    chunk[rows:, 384:512] = meta[...].astype(BF)


def pick_body(cap, rows, scal, *refs):
    count = 8
    chunks = refs[:count]
    mine, other, keys, pack = refs[count:]
    first = (scal[3], scal[4])
    slots = 4 * cap
    line = lax.broadcasted_iota(jnp.int32, (slots, 256), 0).astype(F32)
    for g in range(2):
        sel = []
        for i in range(4):
            ref = chunks[4 * g + i]
            extra = ref[rows:, :]
            pack[4 * g + i] = extra[:, :384]
            meta = extra[:, 384:].astype(F32)
            ids = jnp.concatenate([meta[0:8], meta[8:16]], axis=1)
            pos = jnp.concatenate([meta[16:24], meta[24:32]], axis=1)
            wts = jnp.concatenate([meta[32:40], meta[40:48]], axis=1)
            col = []
            for h in range(2):
                for j in range(2):
                    hit = ids == (first[h] + j).astype(F32)
                    key = (
                        jnp.sum(jnp.where(hit, pos + (1.0 + cap * i), 0.0), axis=0, keepdims=True)
                        - 1.0
                    )
                    wt = jnp.sum(jnp.where(hit, wts, 0.0), axis=0, keepdims=True)
                    n = 2 * h + j
                    keys[4 * g + i, n : n + 1, :] = key
                    keys[4 * g + i, 4 + n : 5 + n, :] = wt
                    col.append(jnp.where(line == key, 1.0, 0.0).astype(BF))
            sel.append(jnp.concatenate(col, axis=0))
        x = jnp.concatenate([chunks[4 * g + i][:256, :] for i in range(4)], axis=0)
        got = jnp.dot(
            jnp.concatenate(sel, axis=1), x, preferred_element_type=F32
        ).astype(BF)
        for j in range(2):
            mine[g, j] = got[slots * j : slots * j + slots]
            other[g, j] = got[slots * (2 + j) : slots * (2 + j) + slots]


def spread_body(dists, scal, own0, own1, par0, par1, gate, up, down):
    z = scal[0]
    core = scal[1]
    size = len(dists)
    for k, dist in enumerate(dists):
        at = lax.rem(z - dist + size, size) * 2
        for pair, who in (((own0, own1), core), ((par0, par1), 1 - core)):
            block = pair[k // 8][k % 8]
            row = at + who
            dst = pl.ds(pl.multiple_of(row * 64, 64), 64)
            gate[dst, :] = block[:, 0:128]
            up[dst, :] = block[:, 128:256]
            ddst = pl.ds(pl.multiple_of(row * 16, 16), 16)
            for c in range(4):
                down[ddst, 128 * c : 128 * c + 128] = block[16 * c : 16 * c + 16, 256:384]


def silu_product(g, u, r):
    v = g * r
    return (v / (1.0 + jnp.exp(-v)) * (u * r)).astype(BF)


def pieces(refs, half, slots):
    own, a, b, c, d = refs

    def block(q, start, size):
        if q < 3:
            return (own, a, b)[q][start : start + size, :]
        if start + size <= half:
            return c[start : start + size, :]
        if start >= half:
            return d[start - half : start - half + size, :]
        return jnp.concatenate([c[start:half, :], d[0 : start + size - half, :]], axis=0)

    return block


def hidden_body(slots, shared, scal, *refs):
    xs = refs[:5]
    if shared:
        gate, up, sgate, sup, out = refs[5:]
    else:
        gate, up, out = refs[5:]
    tp = scal[2]
    half = xs[3].shape[0]
    block = pieces(xs, half, slots)
    order = [lax.rem(tp + s, 4) for s in (0, 3, 1, 2)]

    def product(take, weight):
        total = None
        square = None
        for q in range(4):
            x = take(q)
            at = pl.ds(pl.multiple_of(order[q] * 512, 512), 512)
            part = jnp.dot(x, weight(at), preferred_element_type=F32)
            wide = x.astype(F32)
            sq = wide * wide
            sq = sq[:, 0:128] + sq[:, 128:256] + sq[:, 256:384] + sq[:, 384:512]
            total = part if total is None else total + part
            square = sq if square is None else square + sq
        r = lax.rsqrt(jnp.sum(square, axis=1, keepdims=True) * (1.0 / 2048) + 1e-06)
        return silu_product(total[:, :128], total[:, 128:], r)

    for e in range(2):
        act = product(
            lambda q: jnp.concatenate(
                [block(q, slots * (2 * n + e), slots) for n in range(4)], axis=0
            ),
            lambda at: jnp.concatenate([gate[e, at, :], up[e, at, :]], axis=1),
        )
        for n in range(4):
            r = 2 * n + e
            out[slots * r : slots * r + slots, :] = act[slots * n : slots * n + slots]
    if shared:
        base = 8 * slots
        out[base : base + 2 * slots, :] = product(
            lambda q: block(q, base, 2 * slots),
            lambda at: jnp.concatenate([sgate[at, :], sup[at, :]], axis=1),
        )


def down_body(slots, shared, scal, *refs):
    xs = refs[:5]
    if shared:
        down, sdown, near, far, srows = refs[5:]
    else:
        down, near, far = refs[5:]
    tp = scal[2]
    half = xs[3].shape[0]
    block = pieces(xs, half, slots)
    order = [lax.rem(tp + s, 4) for s in (0, 3, 1, 2)]
    for e in range(2):
        total = None
        for q in range(4):
            x = jnp.concatenate(
                [block(q, slots * (2 * n + e), slots) for n in range(4)], axis=0
            )
            w = down[pl.ds(order[q] * 8, 8), e].reshape(128, 512)
            part = jnp.dot(x, w, preferred_element_type=F32)
            total = part if total is None else total + part
        rows = total.astype(BF)
        for n in range(4):
            (near if n < 2 else far)[n % 2, e] = rows[slots * n : slots * n + slots]
    if shared:
        base = 8 * slots
        total = None
        for q in range(4):
            x = block(q, base, 2 * slots)
            w = sdown[pl.ds(pl.multiple_of(order[q] * 128, 128), 128), :]
            part = jnp.dot(x, w, preferred_element_type=F32)
            total = part if total is None else total + part
        srows[...] = total


def mix_body(rows, slots, near, far, keys, *outs):
    line = lax.broadcasted_iota(jnp.int32, (slots, 256), 0).astype(F32)
    for g in range(2):
        held = jnp.concatenate([near[g, 0], near[g, 1], far[g, 0], far[g, 1]], axis=0)
        for i in range(4):
            b = 4 * g + i
            spread = jnp.concatenate(
                [
                    jnp.where(line == keys[b, n : n + 1, :], keys[b, 4 + n : 5 + n, :], 0.0)
                    for n in range(4)
                ],
                axis=0,
            ).astype(BF)
            dense = lax.dot_general(
                spread, held, (((0,), (0,)), ((), ())), preferred_element_type=F32
            )
            outs[b][...] = dense[:rows].astype(BF)


def per_device(
    sizes,
    tokens,
    routes,
    route_weights,
    norm_gain,
    gate_experts,
    up_experts,
    down_experts,
    shared_gate,
    shared_up,
    shared_down,
):
    groups, zs, tps = sizes
    rows, quarter = tokens.shape
    top = routes.shape[1]
    experts = gate_experts.shape[0]
    cap = 4 * rows * top // (3 * experts)
    slots = 4 * cap
    z = lax.axis_index("z")
    core = lax.axis_index("core")
    tp = lax.axis_index("tp")
    fs = 2 * z + core
    scal = jnp.stack(
        [z, core, tp, 2 * fs, 2 * (2 * z + 1 - core), z, z, z]
    ).astype(jnp.int32)
    FS = ("z", "core")

    (chunk,) = pl.pallas_call(
        pack_body,
        name="pack",
        out_shape=(jax.ShapeDtypeStruct((rows + 64, quarter), BF),),
        in_specs=[VMEM] * 7,
        out_specs=(VMEM,),
        scratch_shapes=[pltpu.VMEM((64, LANES), F32)],
        cost_estimate=pl.CostEstimate(flops=10**7, bytes_accessed=10**6, transcendentals=0),
    )(
        tokens,
        routes.T,
        route_weights.T,
        shared_gate,
        shared_up,
        shared_down,
        norm_gain[:, None],
    )
    held = ring_gather(chunk, "z", zs)

    grp = lax.axis_index("grp")
    parts = groups // 2 if groups % 2 == 0 else 1
    share = gate_experts.shape[1] // parts
    if groups % 2 == 0:
        chosen = jnp.where(grp < parts, gate_experts, up_experts)
        scaled = (chosen * norm_gain[None, :, None]).astype(BF)
        if parts > 1:
            scaled = lax.dynamic_slice_in_dim(scaled, lax.rem(grp, parts) * share, share, 1)
        mine = lax.all_to_all(scaled, FS, 0, 0, tiled=True)
        ring = ring_gather(mine, "grp", groups)
        if groups == 2:
            both = (
                jnp.where(grp == 0, ring[0], ring[1]),
                jnp.where(grp == 0, ring[1], ring[0]),
            )
        else:
            stack = jnp.stack([ring[k if k <= groups // 2 else k - groups] for k in range(groups)])
            placed = [
                lax.dynamic_index_in_dim(stack, lax.rem(grp - g + groups, groups), 0, False)
                for g in range(groups)
            ]
            both = tuple(
                jnp.concatenate(placed[parts * n : parts * n + parts], axis=1) for n in range(2)
            )
    else:
        both = tuple(
            lax.all_to_all((w * norm_gain[None, :, None]).astype(BF), FS, 0, 0, tiled=True)
            for w in (gate_experts, up_experts)
        )
    gate_local, up_local = (
        w.reshape(2 * zs, 2, 64, 128).transpose(1, 0, 2, 3).reshape(2, 128 * zs, 128)
        for w in both
    )
    down_cols = lax.all_to_all(down_experts.astype(BF), FS, 0, 0, tiled=True).reshape(
        2 * zs, 2, 16, 512
    )

    dists = [0]
    for step in range(1, zs // 2 + 1):
        dists.append(step)
        if step < zs - step:
            dists.append(-step)
    halves = (dists[:8], dists[8:])

    def swap(x):
        return shift(x, "core", 2, 1)

    def picked(half):
        return call(
            functools.partial(pick_body, cap, rows),
            "pick",
            [scal],
            [held[d] for d in half],
            [
                jax.ShapeDtypeStruct((2, 2, slots, quarter), BF),
                jax.ShapeDtypeStruct((2, 2, slots, quarter), BF),
                jax.ShapeDtypeStruct((8, 8, 256), F32),
                jax.ShapeDtypeStruct((8, 64, 384), BF),
            ],
            2 * 2 * 448 * 1024 * 512,
        )

    picks = [picked(h) for h in halves]
    packs = [p[3] for p in picks]
    sgate_local, sup_local, sdown_cols = call(
        functools.partial(spread_body, dists),
        "spread",
        [scal],
        packs + [swap(p) for p in packs],
        [
            jax.ShapeDtypeStruct((128 * zs, 128), BF),
            jax.ShapeDtypeStruct((128 * zs, 128), BF),
            jax.ShapeDtypeStruct((32 * zs, 512), BF),
        ],
        10**6,
    )

    dense = {}
    srows = None
    for n in range(2):
        shared = n == 1
        mine, other, keys, _ = picks[n]
        full = [mine.reshape(4 * slots, quarter), swap(other).reshape(4 * slots, quarter)]
        if shared:
            full.append(tokens)
        x = jnp.concatenate(full, axis=0)
        extra = [sgate_local, sup_local] if shared else []
        (act,) = call(
            functools.partial(hidden_body, slots, shared),
            "hidden",
            [scal],
            list(quarters(x, tps)) + [gate_local, up_local] + extra,
            [jax.ShapeDtypeStruct((x.shape[0], 128), BF)],
            2 * x.shape[0] * 2048 * 256,
        )
        outs = [
            jax.ShapeDtypeStruct((2, 2, slots, quarter), BF),
            jax.ShapeDtypeStruct((2, 2, slots, quarter), BF),
        ]
        extra = []
        if shared:
            outs.append(jax.ShapeDtypeStruct((rows, quarter), F32))
            extra = [sdown_cols]
        res = call(
            functools.partial(down_body, slots, shared),
            "down",
            [scal],
            list(quarters(act, tps)) + [down_cols] + extra,
            outs,
            2 * x.shape[0] * 512 * 512,
        )
        if shared:
            srows = res[2]
        blocks = call(
            functools.partial(mix_body, rows, slots),
            "mix",
            [],
            [res[0], swap(res[1]), keys],
            [jax.ShapeDtypeStruct((rows, quarter), BF)] * 8,
            8 * 2 * 256 * 448 * 512,
        )
        for d, block in zip(halves[n], blocks):
            dense[d] = block

    far = zs // 2
    left = dense[far]
    right = dense[-(far - 1)]
    for step in range(far, 0, -1):
        left = shift(left, "z", zs, -1)
        if step > 1:
            left = left + dense[step - 1]
        if step < far:
            right = shift(right, "z", zs, 1)
            if step > 1:
                right = right + dense[-(step - 1)]
    mixed = (
        left.astype(F32) + right.astype(F32) + dense[0].astype(F32) + srows
    ).astype(BF)

    outgoing = jnp.concatenate(
        [
            down_cols.reshape(4, zs // 2, 2, 16, 512).transpose(0, 2, 1, 3, 4).reshape(4, 2, 128, 512),
            sdown_cols.reshape(4, 1, 128, 512),
        ],
        axis=1,
    )
    arrived = lax.all_to_all(outgoing, "tp", 0, 0, tiled=True)
    arrived = arrived.transpose(1, 2, 0, 3).reshape(3, 128, 2048)
    return (
        mixed,
        gate_local,
        up_local,
        arrived[:2],
        sgate_local,
        sup_local,
        arrived[2],
    )


def solution(mesh):
    groups, fs, tps = (mesh.shape[a] for a in ("grp", "fs", "tp"))
    zs = fs // 2
    wide = Mesh(mesh.devices.reshape(groups, zs, 2, tps), ("grp", "z", "core", "tp"))
    fsx = ("z", "core")
    return jax.shard_map(
        functools.partial(per_device, (groups, zs, tps)),
        mesh=wide,
        in_specs=(
            P(("grp", *fsx), "tp"),
            P(("grp", *fsx), None),
            P(("grp", *fsx), None),
            P(fsx),
            P(None, fsx, "tp"),
            P(None, fsx, "tp"),
            P(None, fsx, "tp"),
            P(fsx, "tp"),
            P(fsx, "tp"),
            P(fsx, "tp"),
        ),
        out_specs=(
            P(("grp", *fsx), "tp"),
            P(("grp", *fsx), None, "tp"),
            P(("grp", *fsx), None, "tp"),
            P(("grp", *fsx), "tp", None),
            P("grp", "tp"),
            P("grp", "tp"),
            P(("grp", "tp"), None),
        ),
        check_vma=False,
    )
```

```python
import functools

import jax
import jax.numpy as jnp
from jax import lax
from jax.experimental import pallas as pl
from jax.experimental.pallas import tpu as pltpu
from jax.sharding import Mesh
from jax.sharding import PartitionSpec as P


BF = jnp.bfloat16
F32 = jnp.float32
LANES = 128
VMEM = pl.BlockSpec(memory_space=pltpu.VMEM)
SMEM = pl.BlockSpec(memory_space=pltpu.SMEM)


def call(body, name, scalars, arrays, outs, flops):
    moved = sum(a.size * a.dtype.itemsize for a in arrays) + sum(
        o.size * o.dtype.itemsize for o in outs
    )
    return pl.pallas_call(
        body,
        name=name,
        out_shape=tuple(outs),
        in_specs=[SMEM] * len(scalars) + [VMEM] * len(arrays),
        out_specs=tuple([VMEM] * len(outs)),
        cost_estimate=pl.CostEstimate(flops=flops, bytes_accessed=moved, transcendentals=0),
    )(*scalars, *arrays)


def shift(x, axis, size, by):
    return lax.ppermute(x, axis, [(i, (i + by) % size) for i in range(size)])


def ring_gather(x, axis, size):
    held = {0: x}
    right = left = x
    for step in range(1, size // 2 + 1):
        right = shift(right, axis, size, 1)
        held[step] = right
        if step < size - step:
            left = shift(left, axis, size, -1)
            held[-step] = left
    return held


def quarters(x, size):
    half = x.shape[0] // 2
    a = shift(x, "tp", size, 1)
    b = shift(x, "tp", size, -1)
    c = shift(a[:half], "tp", size, 1)
    d = shift(b[half:], "tp", size, -1)
    return x, a, b, c, d


def pack_body(experts, tok, routes, weights, sgate, sup, sdown, gain, chunk, meta):
    rows = tok.shape[0]
    top = routes.shape[0]
    chunk[:rows, :] = tok[...]
    which = lax.broadcasted_iota(jnp.int32, (experts, rows), 0)
    named = [routes[k : k + 1, :] == which for k in range(top)]
    member = sum(jnp.where(n, 1.0, 0.0) for n in named)
    before = lax.broadcasted_iota(jnp.int32, (rows, rows), 0) < lax.broadcasted_iota(
        jnp.int32, (rows, rows), 1
    )
    count = jnp.dot(
        member.astype(BF), jnp.where(before, 1.0, 0.0).astype(BF), preferred_element_type=F32
    )
    ids = routes[...].astype(F32)
    w = weights[...]
    spare = rows - LANES
    meta[...] = jnp.full(meta.shape, -1.0, F32)
    for k in range(top):
        place = jnp.sum(jnp.where(named[k], count, 0.0), axis=0, keepdims=True)
        meta[16 + k : 17 + k, :] = place[:, :LANES]
        meta[24 + k : 25 + k, :spare] = place[:, LANES:]
    meta[0:top, :] = ids[:, :LANES]
    meta[8 : 8 + top, :spare] = ids[:, LANES:]
    meta[32 : 32 + top, :] = w[:, :LANES]
    meta[40 : 40 + top, :spare] = w[:, LANES:]
    scale = gain[...]
    g = (sgate[...] * scale).astype(BF)
    u = (sup[...] * scale).astype(BF)
    for n in range(2):
        at = slice(32 * n, 32 * n + 32)
        chunk[rows : rows + 32, 128 * n : 128 * n + 128] = g[at]
        chunk[rows : rows + 32, 256 + 128 * n : 384 + 128 * n] = u[at]
    chunk[rows + 32 : rows + 48, :] = sdown[...].astype(BF)
    for n in range(4):
        chunk[rows + 48 : rows + 64, 128 * n : 128 * n + 128] = meta[
            16 * n : 16 * n + 16, :
        ].astype(BF)


def pick_body(cap, rows, count, scal, *refs):
    blocks = refs[:count]
    mine, other, keys, pack = refs[count:]
    first = (scal[3], scal[4])
    slots = 4 * cap
    ngroup = len(blocks) // 4
    line = lax.broadcasted_iota(jnp.int32, (slots, 256), 0).astype(F32)
    shared_at = ngroup * 2 * slots
    for g in range(ngroup):
        sel = []
        for i in range(4):
            b = 4 * g + i
            ref = blocks[b]
            extra = ref[rows : rows + 48, :]
            pack[b] = extra
            other[shared_at + 48 * b : shared_at + 48 * b + 48, :] = extra
            meta = ref[rows + 48 : rows + 64, :].astype(F32)
            ids, pos, wts = (
                jnp.concatenate(
                    [meta[0:8, 128 * n : 128 * n + 128], meta[8:16, 128 * n : 128 * n + 128]],
                    axis=1,
                )
                for n in range(3)
            )
            col = []
            for h in range(2):
                for j in range(2):
                    hit = ids == (first[h] + j).astype(F32)
                    key = (
                        jnp.sum(jnp.where(hit, pos + (1.0 + cap * i), 0.0), axis=0, keepdims=True)
                        - 1.0
                    )
                    wt = jnp.sum(jnp.where(hit, wts, 0.0), axis=0, keepdims=True)
                    n = 2 * h + j
                    keys[b, n : n + 1, :] = key
                    keys[b, 4 + n : 5 + n, :] = wt
                    col.append(jnp.where(line == key, 1.0, 0.0).astype(BF))
            sel.append(jnp.concatenate(col, axis=0))
        x = jnp.concatenate([blocks[4 * g + i][:256, :] for i in range(4)], axis=0)
        got = jnp.dot(jnp.concatenate(sel, axis=1), x, preferred_element_type=F32).astype(BF)
        at = 2 * slots * g
        mine[at : at + 2 * slots, :] = got[: 2 * slots]
        other[at : at + 2 * slots, :] = got[2 * slots :]


def spread_body(dists, scal, own0, own1, par0, par1, gate, up, down):
    z = scal[0]
    core = scal[1]
    size = len(dists)
    count = own0.shape[0]
    for k, dist in enumerate(dists):
        at = lax.rem(z - dist + size, size) * 2
        own, par = (own0, par0) if k < count else (own1, par1)
        n = k if k < count else k - count
        base = par.shape[0] - 48 * own.shape[0] + 48 * n
        for block, who in ((own[n], core), (par[base : base + 48, :], 1 - core)):
            row = at + who
            for m in range(2):
                dst = pl.ds(pl.multiple_of(row * 64 + 32 * m, 32), 32)
                gate[dst, :] = block[0:32, 128 * m : 128 * m + 128]
                up[dst, :] = block[0:32, 256 + 128 * m : 384 + 128 * m]
            down[pl.ds(pl.multiple_of(row * 16, 16), 16), :] = block[32:48, :]


def silu_product(g, u, r):
    v = g * r
    return (v / (1.0 + jnp.exp(-v)) * (u * r)).astype(BF)


def pieces(refs):
    half = refs[3].shape[0]

    def block(q, start, size):
        if q < 3:
            return refs[q][start : start + size, :]
        if start + size <= half:
            return refs[3][start : start + size, :]
        return refs[4][start - half : start - half + size, :]

    return block


def turns(tp):
    return [lax.rem(tp + s, 4) for s in (0, 3, 1, 2)]


def hidden_body(slots, nblock, width, shared, scal, *refs):
    gate, up = refs[5:7]
    out = refs[-1]
    order = turns(scal[2])

    def product(take, weight):
        total = None
        square = None
        for q in range(4):
            x = take(q)
            at = pl.ds(pl.multiple_of(order[q] * 512, 512), 512)
            part = jnp.dot(x, weight(at), preferred_element_type=F32)
            wide = x.astype(F32)
            sq = wide * wide
            sq = sq[:, 0:128] + sq[:, 128:256] + sq[:, 256:384] + sq[:, 384:512]
            total = part if total is None else total + part
            square = sq if square is None else square + sq
        r = lax.rsqrt(jnp.sum(square, axis=1, keepdims=True) * (1.0 / width) + 1e-06)
        return silu_product(total[:, :128], total[:, 128:], r)

    block = pieces(refs[:5])
    for e in range(2):
        act = product(
            lambda q: jnp.concatenate(
                [block(q, slots * r, slots) for r in range(e, nblock, 2)], axis=0
            ),
            lambda at: jnp.concatenate([gate[e, at, :], up[e, at, :]], axis=1),
        )
        for n in range(nblock // 2):
            r = 2 * n + e
            out[slots * r : slots * r + slots, :] = act[slots * n : slots * n + slots]
    if shared:
        sgate, sup = refs[7:9]
        base = nblock * slots
        at0 = refs[9].shape[0] - 2 * slots
        wide_block = pieces(refs[9:14])
        out[base : base + 2 * slots, :] = product(
            lambda q: wide_block(q, at0, 2 * slots),
            lambda at: jnp.concatenate([sgate[at, :], sup[at, :]], axis=1),
        )


def down_body(slots, nblock, shared, scal, *refs):
    downs = refs[5:7]
    block = pieces(refs[:5])
    near, far = refs[8:10] if shared else refs[7:9]
    order = turns(scal[2])
    for e in range(2):
        total = None
        for q in range(4):
            x = jnp.concatenate(
                [block(q, slots * r, slots) for r in range(e, nblock, 2)], axis=0
            )
            w = downs[e][pl.ds(order[q] * 8, 8)].reshape(128, 512)
            part = jnp.dot(x, w, preferred_element_type=F32)
            total = part if total is None else total + part
        rows = total.astype(BF)
        count = nblock // 4
        for n in range(2 * count):
            (near if n < count else far)[n % count, e] = rows[slots * n : slots * n + slots]
    if shared:
        sdown, srows = refs[7], refs[10]
        base = nblock * slots
        total = None
        for q in range(4):
            x = block(q, base, 2 * slots)
            w = sdown[pl.ds(pl.multiple_of(order[q] * 128, 128), 128), :]
            part = jnp.dot(x, w, preferred_element_type=F32)
            total = part if total is None else total + part
        srows[...] = total


def mix_body(rows, slots, near, far, keys, *outs):
    line = lax.broadcasted_iota(jnp.int32, (slots, 256), 0).astype(F32)
    for g in range(near.shape[0]):
        held = jnp.concatenate([near[g, 0], near[g, 1], far[g, 0], far[g, 1]], axis=0)
        for i in range(4):
            b = 4 * g + i
            spread = jnp.concatenate(
                [
                    jnp.where(line == keys[b, n : n + 1, :], keys[b, 4 + n : 5 + n, :], 0.0)
                    for n in range(4)
                ],
                axis=0,
            ).astype(BF)
            dense = lax.dot_general(
                spread, held, (((0,), (0,)), ((), ())), preferred_element_type=F32
            )
            outs[b][...] = dense[:rows].astype(BF)


def place_body(blocks, routed, common):
    width = blocks.shape[3]
    for q in range(blocks.shape[0]):
        at = slice(width * q, width * q + width)
        for n in range(2):
            routed[n, :, at] = blocks[q, n]
        common[:, at] = blocks[q, 2]


def by_group(ring, grp, groups):
    if groups == 2:
        return [jnp.where(grp == g, ring[0], ring[1]) for g in range(2)]
    stack = jnp.stack([ring[k if k <= groups // 2 else k - groups] for k in range(groups)])
    return [
        lax.dynamic_index_in_dim(stack, lax.rem(grp - g + groups, groups), 0, False)
        for g in range(groups)
    ]


def per_device(
    sizes,
    tokens,
    routes,
    route_weights,
    norm_gain,
    gate_experts,
    up_experts,
    down_experts,
    shared_gate,
    shared_up,
    shared_down,
):
    groups, zs, tps = sizes
    rows, quarter = tokens.shape
    top = routes.shape[1]
    experts = gate_experts.shape[0]
    cap = 4 * rows * top // (3 * experts)
    slots = 4 * cap
    z = lax.axis_index("z")
    core = lax.axis_index("core")
    tp = lax.axis_index("tp")
    fs = 2 * z + core
    scal = jnp.stack([z, core, tp, 2 * fs, 2 * (2 * z + 1 - core), z, z, z]).astype(jnp.int32)
    FS = ("z", "core")
    grp = lax.axis_index("grp")
    tie = lax.optimization_barrier

    (chunk,) = pl.pallas_call(
        functools.partial(pack_body, experts),
        name="pack",
        out_shape=(jax.ShapeDtypeStruct((rows + 64, quarter), BF),),
        in_specs=[VMEM] * 7,
        out_specs=(VMEM,),
        scratch_shapes=[pltpu.VMEM((64, LANES), F32)],
        cost_estimate=pl.CostEstimate(flops=10**7, bytes_accessed=10**6, transcendentals=0),
    )(
        tokens,
        routes.T,
        route_weights.T,
        shared_gate,
        shared_up,
        shared_down,
        norm_gain[:, None],
    )
    hops = zs // 2 - 2
    held = {0: chunk}
    right = left = chunk
    for step in range(1, hops + 1):
        held[step] = right = shift(right, "z", zs, 1)
        held[-step] = left = shift(left, "z", zs, -1)

    parts = groups // 2
    share = gate_experts.shape[1] // parts
    scaled = (
        jnp.where(grp < parts, gate_experts, up_experts) * norm_gain[None, :, None]
    ).astype(BF)
    if parts > 1:
        scaled = lax.dynamic_slice_in_dim(scaled, lax.rem(grp, parts) * share, share, 1)
    scaled, right, left = tie((scaled, right, left))
    mine = lax.all_to_all(scaled, FS, 0, 0, tiled=True)
    placed = by_group(ring_gather(mine, "grp", groups), grp, groups)
    gate_local, up_local = (
        jnp.concatenate(placed[parts * n : parts * n + parts], axis=1)
        .reshape(2 * zs, 2, 64, 128)
        .transpose(1, 0, 2, 3)
        .reshape(2, 128 * zs, 128)
        for n in range(2)
    )

    dists = [0]
    for step in range(1, zs // 2 + 1):
        dists.append(step)
        if step < zs - step:
            dists.append(-step)
    cut = 2 * hops
    halves = (dists[:cut], dists[cut:])

    def swap(x):
        return shift(x, "core", 2, 1)

    def picked(arrays):
        count = len(arrays)
        return call(
            functools.partial(pick_body, cap, rows, count),
            "pick",
            [scal],
            arrays,
            [
                jax.ShapeDtypeStruct((count // 4 * 2 * slots, quarter), BF),
                jax.ShapeDtypeStruct((count // 4 * 2 * slots + 48 * count, quarter), BF),
                jax.ShapeDtypeStruct((count, 8, 256), F32),
                jax.ShapeDtypeStruct((count, 48, quarter), BF),
            ],
            count * 448 * 512 * 512,
        )

    picks = [picked([held[d] for d in halves[0]])]
    swaps = [swap(picks[0][1])]
    pair_rows = picks[0][0].shape[0]
    x0 = jnp.concatenate([picks[0][0], swaps[0][:pair_rows], tokens], axis=0)
    half = x0.shape[0] // 2
    a0 = shift(x0, "tp", tps, 1)
    b0 = shift(x0, "tp", tps, -1)
    right, left, a0, b0 = tie((right, left, a0, b0))
    right7 = shift(right, "z", zs, 1)
    left7 = shift(left, "z", zs, -1)
    c0 = shift(a0[:half], "tp", tps, 1)
    d0 = shift(b0[half:], "tp", tps, -1)
    right7, c0, d0 = tie((right7, c0, d0))
    right8 = shift(right7, "z", zs, 1)
    quads = [(x0, a0, b0, c0, d0)]

    dshape = down_experts.shape
    rcut = min(parts, 2)
    ccut = parts // rcut
    dsel = lax.dynamic_index_in_dim(
        down_experts.reshape(dshape[0] // 2, 2, *dshape[1:]), grp // parts, 1, False
    ).astype(BF)
    if parts > 1:
        part = lax.rem(grp, parts)
        rsize, csize = dshape[1] // rcut, dshape[2] // ccut
        dsel = lax.dynamic_slice(
            dsel,
            (0, part // ccut * rsize, lax.rem(part, ccut) * csize),
            (dsel.shape[0], rsize, csize),
        )

    picks.append(picked([left, right7, left7, right8]))
    swaps.append(swap(picks[1][1]))
    pair_rows = picks[1][0].shape[0]
    x1 = jnp.concatenate([picks[1][0], swaps[1][:pair_rows]], axis=0)
    x1, dsel = tie((x1, dsel))
    quads.append(quarters(x1, tps))

    dmine = lax.all_to_all(dsel, FS, 0, 0, tiled=True)
    placed = by_group(ring_gather(dmine, "grp", groups), grp, groups)
    downs = []
    for n in range(2):
        mineset = placed[parts * n : parts * n + parts]
        downs.append(
            jnp.concatenate(
                [
                    jnp.concatenate(mineset[ccut * r : ccut * r + ccut], axis=2)
                    for r in range(rcut)
                ],
                axis=1,
            )
        )

    sgate_local, sup_local, sdown_cols = call(
        functools.partial(spread_body, dists),
        "spread",
        [scal],
        [picks[0][3], picks[1][3], swaps[0], swaps[1]],
        [
            jax.ShapeDtypeStruct((128 * zs, 128), BF),
            jax.ShapeDtypeStruct((128 * zs, 128), BF),
            jax.ShapeDtypeStruct((32 * zs, 512), BF),
        ],
        10**6,
    )

    dense = {}
    srows = None
    for n in range(2):
        shared = n == 1
        nblock = picks[n][0].shape[0] // slots * 2
        arows = nblock * slots + (rows if shared else 0)
        extra = [sgate_local, sup_local, *quads[0]] if shared else []
        (act,) = call(
            functools.partial(hidden_body, slots, nblock, quarter * tps, shared),
            "hidden",
            [scal],
            [*quads[n], gate_local, up_local, *extra],
            [jax.ShapeDtypeStruct((arows, 128), BF)],
            2 * arows * 2048 * 256,
        )
        outs = [jax.ShapeDtypeStruct((nblock // 4, 2, slots, quarter), BF)] * 2
        if shared:
            outs.append(jax.ShapeDtypeStruct((rows, quarter), F32))
        res = call(
            functools.partial(down_body, slots, nblock, shared),
            "down",
            [scal],
            [*quarters(act, tps), *downs, *([sdown_cols] if shared else [])],
            outs,
            2 * arows * 512 * 512,
        )
        if shared:
            srows = res[2]
        count = len(halves[n])
        blocks = call(
            functools.partial(mix_body, rows, slots),
            "mix",
            [],
            [res[0], swap(res[1]), picks[n][2]],
            [jax.ShapeDtypeStruct((rows, quarter), BF)] * count,
            count * 2 * 256 * 448 * 512,
        )
        dense.update(zip(halves[n], blocks))

    def inward(left, right, at):
        return (
            shift(left, "z", zs, -1) + dense[at],
            shift(right, "z", zs, 1) + dense[1 - at],
        )

    far = zs // 2
    left, right = inward(dense[far], dense[1 - far], far - 1)
    d_out = (*downs, sdown_cols)
    left, *d_out = tie((left, *d_out))
    outgoing = jnp.stack([w.reshape(4, 8 * zs, quarter) for w in d_out], axis=1)
    arrived = lax.all_to_all(outgoing, "tp", 0, 0, tiled=True)
    for at in range(far - 2, 1, -1):
        left, right = inward(left, right, at)
    down_local, sdown_local = call(
        place_body,
        "place",
        [],
        [arrived],
        [
            jax.ShapeDtypeStruct((2, 8 * zs, quarter * tps), BF),
            jax.ShapeDtypeStruct((8 * zs, quarter * tps), BF),
        ],
        10**6,
    )
    left, right, down_local, sdown_local = tie((left, right, down_local, sdown_local))
    left, right = inward(left, right, 1)
    left = shift(left, "z", zs, -1)
    mixed = (left.astype(F32) + right.astype(F32) + srows).astype(BF)
    return (
        mixed,
        gate_local,
        up_local,
        down_local,
        sgate_local,
        sup_local,
        sdown_local,
    )


def solution(mesh):
    groups, fs, tps = (mesh.shape[a] for a in ("grp", "fs", "tp"))
    zs = fs // 2
    wide = Mesh(mesh.devices.reshape(groups, zs, 2, tps), ("grp", "z", "core", "tp"))
    fsx = ("z", "core")
    return jax.shard_map(
        functools.partial(per_device, (groups, zs, tps)),
        mesh=wide,
        in_specs=(
            P(("grp", *fsx), "tp"),
            P(("grp", *fsx), None),
            P(("grp", *fsx), None),
            P(fsx),
            P(None, fsx, "tp"),
            P(None, fsx, "tp"),
            P(None, fsx, "tp"),
            P(fsx, "tp"),
            P(fsx, "tp"),
            P(fsx, "tp"),
        ),
        out_specs=(
            P(("grp", *fsx), "tp"),
            P(("grp", *fsx), None, "tp"),
            P(("grp", *fsx), None, "tp"),
            P(("grp", *fsx), "tp", None),
            P("grp", "tp"),
            P("grp", "tp"),
            P(("grp", "tp"), None),
        ),
        check_vma=False,
    )
```

```python
import functools

import jax
import jax.numpy as jnp
from jax import lax
from jax.experimental import pallas as pl
from jax.experimental.pallas import tpu as pltpu
from jax.sharding import Mesh
from jax.sharding import PartitionSpec as P


BF = jnp.bfloat16
F32 = jnp.float32
LANES = 128
VMEM = pl.BlockSpec(memory_space=pltpu.VMEM)
SMEM = pl.BlockSpec(memory_space=pltpu.SMEM)


def call(body, scalars, arrays, outs, flops):
    moved = sum(a.size * a.dtype.itemsize for a in arrays) + sum(
        o.size * o.dtype.itemsize for o in outs
    )
    return pl.pallas_call(
        body,
        out_shape=tuple(outs),
        in_specs=[SMEM] * len(scalars) + [VMEM] * len(arrays),
        out_specs=tuple([VMEM] * len(outs)),
        cost_estimate=pl.CostEstimate(flops=flops, bytes_accessed=moved, transcendentals=0),
    )(*scalars, *arrays)


def shift(x, axis, size, by):
    return lax.ppermute(x, axis, [(i, (i + by) % size) for i in range(size)])


def ring_gather(x, axis, size):
    held = {0: x}
    right = left = x
    for step in range(1, size // 2 + 1):
        right = shift(right, axis, size, 1)
        held[step] = right
        if step < size - step:
            left = shift(left, axis, size, -1)
            held[-step] = left
    return held


def quarters(x, size):
    half = x.shape[0] // 2
    a = shift(x, "tp", size, 1)
    b = shift(x, "tp", size, -1)
    c = shift(a[:half], "tp", size, 1)
    d = shift(b[half:], "tp", size, -1)
    return x, a, b, c, d


def pack_body(experts, tok, routes, weights, sgate, sup, sdown, gain, chunk, meta):
    rows = tok.shape[0]
    top = routes.shape[0]
    chunk[:rows, :] = tok[...]
    which = lax.broadcasted_iota(jnp.int32, (experts, rows), 0)
    named = [routes[k : k + 1, :] == which for k in range(top)]
    member = sum(jnp.where(n, 1.0, 0.0) for n in named)
    before = lax.broadcasted_iota(jnp.int32, (rows, rows), 0) < lax.broadcasted_iota(
        jnp.int32, (rows, rows), 1
    )
    count = jnp.dot(
        member.astype(BF), jnp.where(before, 1.0, 0.0).astype(BF), preferred_element_type=F32
    )
    ids = routes[...].astype(F32)
    w = weights[...]
    spare = rows - LANES
    meta[...] = jnp.full(meta.shape, -1.0, F32)
    for k in range(top):
        place = jnp.sum(jnp.where(named[k], count, 0.0), axis=0, keepdims=True)
        meta[16 + k : 17 + k, :] = place[:, :LANES]
        meta[24 + k : 25 + k, :spare] = place[:, LANES:]
    meta[0:top, :] = ids[:, :LANES]
    meta[8 : 8 + top, :spare] = ids[:, LANES:]
    meta[32 : 32 + top, :] = w[:, :LANES]
    meta[40 : 40 + top, :spare] = w[:, LANES:]
    scale = jnp.transpose(jnp.broadcast_to(gain[...], (8, 64)))[:, :1]
    g = (sgate[...] * scale).astype(BF)
    u = (sup[...] * scale).astype(BF)
    for n in range(2):
        at = slice(32 * n, 32 * n + 32)
        chunk[rows : rows + 32, 128 * n : 128 * n + 128] = g[at]
        chunk[rows : rows + 32, 256 + 128 * n : 384 + 128 * n] = u[at]
    chunk[rows + 32 : rows + 48, :] = sdown[...].astype(BF)
    for n in range(4):
        chunk[rows + 48 : rows + 64, 128 * n : 128 * n + 128] = meta[
            16 * n : 16 * n + 16, :
        ].astype(BF)


def pick_body(cap, rows, count, scal, *refs):
    blocks = refs[:count]
    mine, other, keys, pack = refs[count:]
    first = (scal[3], scal[4])
    slots = 4 * cap
    ngroup = len(blocks) // 4
    line = lax.broadcasted_iota(jnp.int32, (slots, 256), 0).astype(F32)
    shared_at = ngroup * 2 * slots
    for g in range(ngroup):
        sel = []
        for i in range(4):
            b = 4 * g + i
            ref = blocks[b]
            extra = ref[rows : rows + 48, :]
            pack[b] = extra
            other[shared_at + 48 * b : shared_at + 48 * b + 48, :] = extra
            meta = ref[rows + 48 : rows + 64, :].astype(F32)
            ids, pos, wts = (
                jnp.concatenate(
                    [meta[0:8, 128 * n : 128 * n + 128], meta[8:16, 128 * n : 128 * n + 128]],
                    axis=1,
                )
                for n in range(3)
            )
            col = []
            for h in range(2):
                for j in range(2):
                    hit = ids == (first[h] + j).astype(F32)
                    key = (
                        jnp.sum(jnp.where(hit, pos + (1.0 + cap * i), 0.0), axis=0, keepdims=True)
                        - 1.0
                    )
                    wt = jnp.sum(jnp.where(hit, wts, 0.0), axis=0, keepdims=True)
                    n = 2 * h + j
                    keys[b, n : n + 1, :] = key
                    keys[b, 4 + n : 5 + n, :] = wt
                    col.append(jnp.where(line == key, 1.0, 0.0).astype(BF))
            sel.append(jnp.concatenate(col, axis=0))
        x = jnp.concatenate([blocks[4 * g + i][:256, :] for i in range(4)], axis=0)
        got = jnp.dot(jnp.concatenate(sel, axis=1), x, preferred_element_type=F32).astype(BF)
        at = 2 * slots * g
        mine[at : at + 2 * slots, :] = got[: 2 * slots]
        other[at : at + 2 * slots, :] = got[2 * slots :]


def spread_body(dists, scal, own0, own1, par0, par1, gate, up, down):
    z = scal[0]
    core = scal[1]
    size = len(dists)
    count = own0.shape[0]
    for k, dist in enumerate(dists):
        at = lax.rem(z - dist + size, size) * 2
        own, par = (own0, par0) if k < count else (own1, par1)
        n = k if k < count else k - count
        base = par.shape[0] - 48 * own.shape[0] + 48 * n
        for block, who in ((own[n], core), (par[base : base + 48, :], 1 - core)):
            row = at + who
            for m in range(2):
                dst = pl.ds(pl.multiple_of(row * 64 + 32 * m, 32), 32)
                gate[dst, :] = block[0:32, 128 * m : 128 * m + 128]
                up[dst, :] = block[0:32, 256 + 128 * m : 384 + 128 * m]
            down[pl.ds(pl.multiple_of(row * 16, 16), 16), :] = block[32:48, :]


def silu_product(g, u, r):
    v = g * r
    return (v / (1.0 + jnp.exp(-v)) * (u * r)).astype(BF)


def pieces(refs):
    half = refs[3].shape[0]

    def block(q, start, size):
        if q < 3:
            return refs[q][start : start + size, :]
        if start + size <= half:
            return refs[3][start : start + size, :]
        return refs[4][start - half : start - half + size, :]

    return block


def turns(tp):
    return [lax.rem(tp + s, 4) for s in (0, 3, 1, 2)]


def hidden_body(slots, nblock, width, shared, scal, *refs):
    gate, up = refs[5:7]
    out = refs[-1]
    order = turns(scal[2])

    def product(take, weight):
        total = None
        square = None
        for q in range(4):
            x = take(q)
            at = pl.ds(pl.multiple_of(order[q] * 512, 512), 512)
            part = jnp.dot(x, weight(at), preferred_element_type=F32)
            wide = x.astype(F32)
            sq = wide * wide
            sq = sq[:, 0:128] + sq[:, 128:256] + sq[:, 256:384] + sq[:, 384:512]
            total = part if total is None else total + part
            square = sq if square is None else square + sq
        r = lax.rsqrt(jnp.sum(square, axis=1, keepdims=True) * (1.0 / width) + 1e-06)
        return silu_product(total[:, :128], total[:, 128:], r)

    block = pieces(refs[:5])
    for e in range(2):
        act = product(
            lambda q: jnp.concatenate(
                [block(q, slots * r, slots) for r in range(e, nblock, 2)], axis=0
            ),
            lambda at: jnp.concatenate([gate[e, at, :], up[e, at, :]], axis=1),
        )
        for n in range(nblock // 2):
            r = 2 * n + e
            out[slots * r : slots * r + slots, :] = act[slots * n : slots * n + slots]
    if shared:
        sgate, sup = refs[7:9]
        base = nblock * slots
        at0 = refs[9].shape[0] - 2 * slots
        wide_block = pieces(refs[9:14])
        out[base : base + 2 * slots, :] = product(
            lambda q: wide_block(q, at0, 2 * slots),
            lambda at: jnp.concatenate([sgate[at, :], sup[at, :]], axis=1),
        )


def down_body(slots, nblock, shared, scal, *refs):
    downs = refs[5:7]
    block = pieces(refs[:5])
    near, far = refs[8:10] if shared else refs[7:9]
    order = turns(scal[2])
    for e in range(2):
        total = None
        for q in range(4):
            x = jnp.concatenate(
                [block(q, slots * r, slots) for r in range(e, nblock, 2)], axis=0
            )
            w = downs[e][pl.ds(order[q] * 8, 8)].reshape(128, 512)
            part = jnp.dot(x, w, preferred_element_type=F32)
            total = part if total is None else total + part
        rows = total.astype(BF)
        count = nblock // 4
        for n in range(2 * count):
            (near if n < count else far)[n % count, e] = rows[slots * n : slots * n + slots]
    if shared:
        sdown, srows = refs[7], refs[10]
        base = nblock * slots
        total = None
        for q in range(4):
            x = block(q, base, 2 * slots)
            w = sdown[pl.ds(pl.multiple_of(order[q] * 128, 128), 128), :]
            part = jnp.dot(x, w, preferred_element_type=F32)
            total = part if total is None else total + part
        srows[...] = total


def mix_body(rows, slots, near, far, keys, *outs):
    line = lax.broadcasted_iota(jnp.int32, (slots, 256), 0).astype(F32)
    for g in range(near.shape[0]):
        held = jnp.concatenate([near[g, 0], near[g, 1], far[g, 0], far[g, 1]], axis=0)
        for i in range(4):
            b = 4 * g + i
            spread = jnp.concatenate(
                [
                    jnp.where(line == keys[b, n : n + 1, :], keys[b, 4 + n : 5 + n, :], 0.0)
                    for n in range(4)
                ],
                axis=0,
            ).astype(BF)
            dense = lax.dot_general(
                spread, held, (((0,), (0,)), ((), ())), preferred_element_type=F32
            )
            outs[b][...] = dense[:rows].astype(BF)


def place_body(blocks, routed, common):
    width = blocks.shape[3]
    for q in range(blocks.shape[0]):
        at = slice(width * q, width * q + width)
        for n in range(2):
            routed[n, :, at] = blocks[q, n]
        common[:, at] = blocks[q, 2]


def by_group(ring, grp, groups):
    if groups == 2:
        return [jnp.where(grp == g, ring[0], ring[1]) for g in range(2)]
    stack = jnp.stack([ring[k if k <= groups // 2 else k - groups] for k in range(groups)])
    return [
        lax.dynamic_index_in_dim(stack, lax.rem(grp - g + groups, groups), 0, False)
        for g in range(groups)
    ]


def layer(
    sizes,
    tokens,
    routes,
    route_weights,
    norm_gain,
    gate_experts,
    up_experts,
    down_experts,
    shared_gate,
    shared_up,
    shared_down,
):
    groups, zs, tps = sizes
    rows, quarter = tokens.shape
    top = routes.shape[1]
    experts = gate_experts.shape[0]
    cap = 4 * rows * top // (3 * experts)
    slots = 4 * cap
    z = lax.axis_index("z")
    core = lax.axis_index("core")
    tp = lax.axis_index("tp")
    fs = 2 * z + core
    scal = jnp.stack([z, core, tp, 2 * fs, 2 * (2 * z + 1 - core), z, z, z]).astype(jnp.int32)
    FS = ("z", "core")
    grp = lax.axis_index("grp")
    tie = lax.optimization_barrier

    (chunk,) = pl.pallas_call(
        functools.partial(pack_body, experts),
        name="pack",
        out_shape=(jax.ShapeDtypeStruct((rows + 64, quarter), BF),),
        in_specs=[VMEM] * 7,
        out_specs=(VMEM,),
        scratch_shapes=[pltpu.VMEM((64, LANES), F32)],
        cost_estimate=pl.CostEstimate(flops=10**7, bytes_accessed=10**6, transcendentals=0),
    )(
        tokens,
        routes.T,
        route_weights.T,
        shared_gate,
        shared_up,
        shared_down,
        norm_gain[None, :],
    )
    hops = zs // 2 - 2
    held = {0: chunk}
    right = left = chunk
    for step in range(1, hops + 1):
        held[step] = right = shift(right, "z", zs, 1)
        held[-step] = left = shift(left, "z", zs, -1)

    parts = groups // 2
    share = gate_experts.shape[1] // parts
    scaled = (
        jnp.where(grp < parts, gate_experts, up_experts) * norm_gain[None, :, None]
    ).astype(BF)
    if parts > 1:
        scaled = lax.dynamic_slice_in_dim(scaled, lax.rem(grp, parts) * share, share, 1)
    scaled, right, left = tie((scaled, right, left))
    held[hops], held[-hops] = right, left
    mine = lax.all_to_all(scaled, FS, 0, 0, tiled=True)

    dists = [0]
    for step in range(1, zs // 2 + 1):
        dists.append(step)
        if step < zs - step:
            dists.append(-step)
    cut = 2 * hops
    halves = (dists[:cut], dists[cut:])

    def swap(x):
        return shift(x, "core", 2, 1)

    def picked(arrays):
        count = len(arrays)
        return call(
            functools.partial(pick_body, cap, rows, count),
            [scal],
            arrays,
            [
                jax.ShapeDtypeStruct((count // 4 * 2 * slots, quarter), BF),
                jax.ShapeDtypeStruct((count // 4 * 2 * slots + 48 * count, quarter), BF),
                jax.ShapeDtypeStruct((count, 8, 256), F32),
                jax.ShapeDtypeStruct((count, 48, quarter), BF),
            ],
            count * 448 * 512 * 512,
        )

    picks = [picked([held[d] for d in halves[0]])]
    swaps = [swap(picks[0][1])]
    pair_rows = picks[0][0].shape[0]
    x0 = jnp.concatenate([picks[0][0], swaps[0][:pair_rows], tokens], axis=0)
    half = x0.shape[0] // 2
    a0 = shift(x0, "tp", tps, 1)
    b0 = shift(x0, "tp", tps, -1)
    right, left, a0, b0, mine = tie((right, left, a0, b0, mine))
    ring = ring_gather(mine, "grp", groups)
    placed = by_group(ring, grp, groups)
    gate_local, up_local = (
        jnp.concatenate(placed[parts * n : parts * n + parts], axis=1)
        .reshape(2 * zs, 2, 64, 128)
        .transpose(1, 0, 2, 3)
        .reshape(2, 128 * zs, 128)
        for n in range(2)
    )
    right7 = shift(right, "z", zs, 1)
    left7 = shift(left, "z", zs, -1)
    c0 = shift(a0[:half], "tp", tps, 1)
    d0 = shift(b0[half:], "tp", tps, -1)
    right7, c0, d0 = tie((right7, c0, d0))
    right8 = shift(right7, "z", zs, 1)
    quads = [(x0, a0, b0, c0, d0)]

    dshape = down_experts.shape
    rcut = min(parts, 2)
    ccut = parts // rcut
    dsel = lax.dynamic_index_in_dim(
        down_experts.reshape(dshape[0] // 2, 2, *dshape[1:]), grp // parts, 1, False
    ).astype(BF)
    if parts > 1:
        part = lax.rem(grp, parts)
        rsize, csize = dshape[1] // rcut, dshape[2] // ccut
        dsel = lax.dynamic_slice(
            dsel,
            (0, part // ccut * rsize, lax.rem(part, ccut) * csize),
            (dsel.shape[0], rsize, csize),
        )

    dsel, c0, d0 = tie((dsel, c0, d0))
    quads = [(x0, a0, b0, c0, d0)]
    picks.append(picked([left, right7, left7, right8]))
    swaps.append(swap(picks[1][1]))
    pair_rows = picks[1][0].shape[0]
    x1 = jnp.concatenate([picks[1][0], swaps[1][:pair_rows]], axis=0)
    quads.append(quarters(x1, tps))

    dmine = lax.all_to_all(dsel, FS, 0, 0, tiled=True)
    ring = ring_gather(dmine, "grp", groups)
    placed = by_group(ring, grp, groups)
    downs = []
    for n in range(2):
        mineset = placed[parts * n : parts * n + parts]
        downs.append(
            jnp.concatenate(
                [
                    jnp.concatenate(mineset[ccut * r : ccut * r + ccut], axis=2)
                    for r in range(rcut)
                ],
                axis=1,
            )
        )

    sgate_local, sup_local, sdown_cols = call(
        functools.partial(spread_body, dists),
        [scal],
        [picks[0][3], picks[1][3], swaps[0], swaps[1]],
        [
            jax.ShapeDtypeStruct((128 * zs, 128), BF),
            jax.ShapeDtypeStruct((128 * zs, 128), BF),
            jax.ShapeDtypeStruct((32 * zs, 512), BF),
        ],
        10**6,
    )

    dense = {}
    srows = None
    for n in range(2):
        shared = n == 1
        nblock = picks[n][0].shape[0] // slots * 2
        arows = nblock * slots + (rows if shared else 0)
        extra = [sgate_local, sup_local, *quads[0]] if shared else []
        (act,) = call(
            functools.partial(hidden_body, slots, nblock, quarter * tps, shared),
            [scal],
            [*quads[n], gate_local, up_local, *extra],
            [jax.ShapeDtypeStruct((arows, 128), BF)],
            2 * arows * 2048 * 256,
        )
        outs = [jax.ShapeDtypeStruct((nblock // 4, 2, slots, quarter), BF)] * 2
        if shared:
            outs.append(jax.ShapeDtypeStruct((rows, quarter), F32))
        res = call(
            functools.partial(down_body, slots, nblock, shared),
            [scal],
            [*quarters(act, tps), *downs, *([sdown_cols] if shared else [])],
            outs,
            2 * arows * 512 * 512,
        )
        if shared:
            srows = res[2]
        count = len(halves[n])
        blocks = call(
            functools.partial(mix_body, rows, slots),
            [],
            [res[0], swap(res[1]), picks[n][2]],
            [jax.ShapeDtypeStruct((rows, quarter), BF)] * count,
            count * 2 * 256 * 448 * 512,
        )
        dense.update(zip(halves[n], blocks))

    def inward(left, right, at):
        left = shift(left, "z", zs, -1)
        return left + dense[at], shift(right, "z", zs, 1) + dense[1 - at]

    far = zs // 2
    left, right = inward(dense[far], dense[1 - far], far - 1)
    outgoing = jnp.stack(
        [w.reshape(4, 8 * zs, quarter) for w in (*downs, sdown_cols)], axis=1
    )
    arrived = lax.all_to_all(outgoing, "tp", 0, 0, tiled=True)
    for at in range(far - 2, 0, -1):
        left, right = inward(left, right, at)
    down_local, sdown_local = call(
        place_body,
        [],
        [arrived],
        [
            jax.ShapeDtypeStruct((2, 8 * zs, quarter * tps), BF),
            jax.ShapeDtypeStruct((8 * zs, quarter * tps), BF),
        ],
        10**6,
    )
    left = shift(left, "z", zs, -1)
    mixed = (left.astype(F32) + right.astype(F32) + srows).astype(BF)
    return (
        mixed,
        gate_local,
        up_local,
        down_local,
        sgate_local,
        sup_local,
        sdown_local,
    )


def solution(mesh):
    groups, fs, tps = (mesh.shape[a] for a in ("grp", "fs", "tp"))
    zs = fs // 2
    wide = Mesh(mesh.devices.reshape(groups, zs, 2, tps), ("grp", "z", "core", "tp"))
    fsx = ("z", "core")
    return jax.shard_map(
        functools.partial(layer, (groups, zs, tps)),
        mesh=wide,
        in_specs=(
            P(("grp", *fsx), "tp"),
            P(("grp", *fsx), None),
            P(("grp", *fsx), None),
            P(fsx),
            P(None, fsx, "tp"),
            P(None, fsx, "tp"),
            P(None, fsx, "tp"),
            P(fsx, "tp"),
            P(fsx, "tp"),
            P(fsx, "tp"),
        ),
        out_specs=(
            P(("grp", *fsx), "tp"),
            P(("grp", *fsx), None, "tp"),
            P(("grp", *fsx), None, "tp"),
            P(("grp", *fsx), "tp", None),
            P("grp", "tp"),
            P("grp", "tp"),
            P(("grp", "tp"), None),
        ),
        check_vma=False,
    )
```

```python
import functools

import jax
import jax.numpy as jnp
from jax import lax
from jax.experimental import pallas as pl
from jax.experimental.pallas import tpu as pltpu
from jax.sharding import Mesh
from jax.sharding import PartitionSpec as P


BF = jnp.bfloat16
F32 = jnp.float32
LANES = 128
VMEM = pl.BlockSpec(memory_space=pltpu.VMEM)
SMEM = pl.BlockSpec(memory_space=pltpu.SMEM)


def call(body, scalars, arrays, outs, flops):
    moved = sum(a.size * a.dtype.itemsize for a in arrays) + sum(
        o.size * o.dtype.itemsize for o in outs
    )
    return pl.pallas_call(
        body,
        out_shape=tuple(outs),
        in_specs=[SMEM] * len(scalars) + [VMEM] * len(arrays),
        out_specs=tuple([VMEM] * len(outs)),
        cost_estimate=pl.CostEstimate(flops=flops, bytes_accessed=moved, transcendentals=0),
    )(*scalars, *arrays)


def shift(x, axis, size, by):
    return lax.ppermute(x, axis, [(i, (i + by) % size) for i in range(size)])


def ring_gather(x, axis, size):
    held = {0: x}
    right = left = x
    for step in range(1, size // 2 + 1):
        right = shift(right, axis, size, 1)
        held[step] = right
        if step < size - step:
            left = shift(left, axis, size, -1)
            held[-step] = left
    return held


def quarters(x, size):
    half = x.shape[0] // 2
    a = shift(x, "tp", size, 1)
    b = shift(x, "tp", size, -1)
    c = shift(a[:half], "tp", size, 1)
    d = shift(b[half:], "tp", size, -1)
    return x, a, b, c, d


def pack_body(experts, tok, routes, weights, sgate, sup, sdown, gain, chunk, meta):
    rows = tok.shape[0]
    top = routes.shape[0]
    chunk[:rows, :] = tok[...]
    which = lax.broadcasted_iota(jnp.int32, (experts, rows), 0)
    named = [routes[k : k + 1, :] == which for k in range(top)]
    member = sum(jnp.where(n, 1.0, 0.0) for n in named)
    before = lax.broadcasted_iota(jnp.int32, (rows, rows), 0) < lax.broadcasted_iota(
        jnp.int32, (rows, rows), 1
    )
    count = jnp.dot(
        member.astype(BF), jnp.where(before, 1.0, 0.0).astype(BF), preferred_element_type=F32
    )
    ids = routes[...].astype(F32)
    w = weights[...]
    spare = rows - LANES
    meta[...] = jnp.full(meta.shape, -1.0, F32)
    for k in range(top):
        place = jnp.sum(jnp.where(named[k], count, 0.0), axis=0, keepdims=True)
        meta[16 + k : 17 + k, :] = place[:, :LANES]
        meta[24 + k : 25 + k, :spare] = place[:, LANES:]
    meta[0:top, :] = ids[:, :LANES]
    meta[8 : 8 + top, :spare] = ids[:, LANES:]
    meta[32 : 32 + top, :] = w[:, :LANES]
    meta[40 : 40 + top, :spare] = w[:, LANES:]
    scale = jnp.transpose(jnp.broadcast_to(gain[...], (8, 64)))[:, :1]
    g = (sgate[...] * scale).astype(BF)
    u = (sup[...] * scale).astype(BF)
    for n in range(2):
        at = slice(32 * n, 32 * n + 32)
        chunk[rows : rows + 32, 128 * n : 128 * n + 128] = g[at]
        chunk[rows : rows + 32, 256 + 128 * n : 384 + 128 * n] = u[at]
    chunk[rows + 32 : rows + 48, :] = sdown[...].astype(BF)
    for n in range(4):
        chunk[rows + 48 : rows + 64, 128 * n : 128 * n + 128] = meta[
            16 * n : 16 * n + 16, :
        ].astype(BF)


def pick_body(cap, rows, count, scal, *refs):
    blocks = refs[:count]
    mine, other, keys, pack = refs[count:]
    first = (scal[3], scal[4])
    slots = 4 * cap
    ngroup = len(blocks) // 4
    line = lax.broadcasted_iota(jnp.int32, (slots, 256), 0).astype(F32)
    shared_at = ngroup * 2 * slots
    for g in range(ngroup):
        sel = []
        for i in range(4):
            b = 4 * g + i
            ref = blocks[b]
            extra = ref[rows : rows + 48, :]
            pack[b] = extra
            other[shared_at + 48 * b : shared_at + 48 * b + 48, :] = extra
            meta = ref[rows + 48 : rows + 64, :].astype(F32)
            ids, pos, wts = (
                jnp.concatenate(
                    [meta[0:8, 128 * n : 128 * n + 128], meta[8:16, 128 * n : 128 * n + 128]],
                    axis=1,
                )
                for n in range(3)
            )
            col = []
            for h in range(2):
                for j in range(2):
                    hit = ids == (first[h] + j).astype(F32)
                    key = (
                        jnp.sum(jnp.where(hit, pos + (1.0 + cap * i), 0.0), axis=0, keepdims=True)
                        - 1.0
                    )
                    wt = jnp.sum(jnp.where(hit, wts, 0.0), axis=0, keepdims=True)
                    n = 2 * h + j
                    keys[b, n : n + 1, :] = key
                    keys[b, 4 + n : 5 + n, :] = wt
                    col.append(jnp.where(line == key, 1.0, 0.0).astype(BF))
            sel.append(jnp.concatenate(col, axis=0))
        x = jnp.concatenate([blocks[4 * g + i][:256, :] for i in range(4)], axis=0)
        got = jnp.dot(jnp.concatenate(sel, axis=1), x, preferred_element_type=F32).astype(BF)
        at = 2 * slots * g
        mine[at : at + 2 * slots, :] = got[: 2 * slots]
        other[at : at + 2 * slots, :] = got[2 * slots :]


def spread_body(dists, scal, own0, own1, par0, par1, gate, up, down):
    z = scal[0]
    core = scal[1]
    size = len(dists)
    count = own0.shape[0]
    for k, dist in enumerate(dists):
        at = lax.rem(z - dist + size, size) * 2
        own, par = (own0, par0) if k < count else (own1, par1)
        n = k if k < count else k - count
        base = par.shape[0] - 48 * own.shape[0] + 48 * n
        for block, who in ((own[n], core), (par[base : base + 48, :], 1 - core)):
            row = at + who
            for m in range(2):
                dst = pl.ds(pl.multiple_of(row * 64 + 32 * m, 32), 32)
                gate[dst, :] = block[0:32, 128 * m : 128 * m + 128]
                up[dst, :] = block[0:32, 256 + 128 * m : 384 + 128 * m]
            down[pl.ds(pl.multiple_of(row * 16, 16), 16), :] = block[32:48, :]


def silu_product(g, u, r):
    v = g * r
    return (v / (1.0 + jnp.exp(-v)) * (u * r)).astype(BF)


def pieces(refs):
    half = refs[-1].shape[0]

    def block(q, start, size):
        if q < 3 and len(refs) == 5:
            return refs[q][start : start + size, :]
        first = refs[-2] if q == 3 else refs[2 * q]
        second = refs[-1] if q == 3 else refs[2 * q + 1]
        if start + size <= half:
            return first[start : start + size, :]
        return second[start - half : start - half + size, :]

    return block


def turns(tp):
    return [lax.rem(tp + s, 4) for s in (0, 3, 1, 2)]


def hidden_body(slots, nblock, nx, width, shared, scal, *refs):
    gate, up = refs[nx : nx + 2]
    out = refs[-1]
    order = turns(scal[2])

    def product(take, weight):
        total = None
        square = None
        for q in range(4):
            x = take(q)
            at = pl.ds(pl.multiple_of(order[q] * 512, 512), 512)
            part = jnp.dot(x, weight(at), preferred_element_type=F32)
            wide = x.astype(F32)
            sq = wide * wide
            sq = sq[:, 0:128] + sq[:, 128:256] + sq[:, 256:384] + sq[:, 384:512]
            total = part if total is None else total + part
            square = sq if square is None else square + sq
        r = lax.rsqrt(jnp.sum(square, axis=1, keepdims=True) * (1.0 / width) + 1e-06)
        return silu_product(total[:, :128], total[:, 128:], r)

    block = pieces(refs[:nx])
    for e in range(2):
        act = product(
            lambda q: jnp.concatenate(
                [block(q, slots * r, slots) for r in range(e, nblock, 2)], axis=0
            ),
            lambda at: jnp.concatenate([gate[e, at, :], up[e, at, :]], axis=1),
        )
        for n in range(nblock // 2):
            r = 2 * n + e
            out[slots * r : slots * r + slots, :] = act[slots * n : slots * n + slots]
    if shared:
        sgate, sup = refs[nx + 2 : nx + 4]
        base = nblock * slots
        wide_block = pieces(refs[nx + 4 : -1])
        at0 = 2 * refs[-2].shape[0] - 2 * slots
        out[base : base + 2 * slots, :] = product(
            lambda q: wide_block(q, at0, 2 * slots),
            lambda at: jnp.concatenate([sgate[at, :], sup[at, :]], axis=1),
        )


def down_body(slots, nblock, shared, scal, *refs):
    downs = refs[5:7]
    block = pieces(refs[:5])
    near, far = refs[8:10] if shared else refs[7:9]
    order = turns(scal[2])
    for e in range(2):
        total = None
        for q in range(4):
            x = jnp.concatenate(
                [block(q, slots * r, slots) for r in range(e, nblock, 2)], axis=0
            )
            w = downs[e][pl.ds(order[q] * 8, 8)].reshape(128, 512)
            part = jnp.dot(x, w, preferred_element_type=F32)
            total = part if total is None else total + part
        rows = total.astype(BF)
        count = nblock // 4
        for n in range(2 * count):
            (near if n < count else far)[n % count, e] = rows[slots * n : slots * n + slots]
    if shared:
        sdown, srows = refs[7], refs[10]
        base = nblock * slots
        total = None
        for q in range(4):
            x = block(q, base, 2 * slots)
            w = sdown[pl.ds(pl.multiple_of(order[q] * 128, 128), 128), :]
            part = jnp.dot(x, w, preferred_element_type=F32)
            total = part if total is None else total + part
        srows[...] = total


def mix_body(rows, slots, near, far, keys, *outs):
    line = lax.broadcasted_iota(jnp.int32, (slots, 256), 0).astype(F32)
    for g in range(near.shape[0]):
        held = jnp.concatenate([near[g, 0], near[g, 1], far[g, 0], far[g, 1]], axis=0)
        for i in range(4):
            b = 4 * g + i
            spread = jnp.concatenate(
                [
                    jnp.where(line == keys[b, n : n + 1, :], keys[b, 4 + n : 5 + n, :], 0.0)
                    for n in range(4)
                ],
                axis=0,
            ).astype(BF)
            dense = lax.dot_general(
                spread, held, (((0,), (0,)), ((), ())), preferred_element_type=F32
            )
            outs[b][...] = dense[:rows].astype(BF)


def place_body(blocks, routed, common):
    width = blocks.shape[3]
    for q in range(blocks.shape[0]):
        at = slice(width * q, width * q + width)
        for n in range(2):
            routed[n, :, at] = blocks[q, n]
        common[:, at] = blocks[q, 2]


def by_group(ring, grp, groups):
    if groups == 2:
        return [jnp.where(grp == g, ring[0], ring[1]) for g in range(2)]
    stack = jnp.stack([ring[k if k <= groups // 2 else k - groups] for k in range(groups)])
    return [
        lax.dynamic_index_in_dim(stack, lax.rem(grp - g + groups, groups), 0, False)
        for g in range(groups)
    ]


def layer(
    sizes,
    tokens,
    routes,
    route_weights,
    norm_gain,
    gate_experts,
    up_experts,
    down_experts,
    shared_gate,
    shared_up,
    shared_down,
):
    groups, zs, tps = sizes
    rows, quarter = tokens.shape
    top = routes.shape[1]
    experts = gate_experts.shape[0]
    cap = 4 * rows * top // (3 * experts)
    slots = 4 * cap
    z = lax.axis_index("z")
    core = lax.axis_index("core")
    tp = lax.axis_index("tp")
    fs = 2 * z + core
    scal = jnp.stack([z, core, tp, 2 * fs, 2 * (2 * z + 1 - core), z, z, z]).astype(jnp.int32)
    FS = ("z", "core")
    grp = lax.axis_index("grp")
    tie = lax.optimization_barrier

    (chunk,) = pl.pallas_call(
        functools.partial(pack_body, experts),
        name="pack",
        out_shape=(jax.ShapeDtypeStruct((rows + 64, quarter), BF),),
        in_specs=[VMEM] * 7,
        out_specs=(VMEM,),
        scratch_shapes=[pltpu.VMEM((64, LANES), F32)],
        cost_estimate=pl.CostEstimate(flops=10**7, bytes_accessed=10**6, transcendentals=0),
    )(
        tokens,
        routes.T,
        route_weights.T,
        shared_gate,
        shared_up,
        shared_down,
        norm_gain[None, :],
    )
    hops = zs // 2 - 2
    held = {0: chunk}
    right = left = chunk
    for step in range(1, hops + 1):
        held[step] = right = shift(right, "z", zs, 1)
        held[-step] = left = shift(left, "z", zs, -1)

    parts = groups // 2
    share = gate_experts.shape[1] // parts
    scaled = (
        jnp.where(grp < parts, gate_experts, up_experts) * norm_gain[None, :, None]
    ).astype(BF)
    if parts > 1:
        scaled = lax.dynamic_slice_in_dim(scaled, lax.rem(grp, parts) * share, share, 1)
    held[hops], held[-hops] = tie((right, left))
    right, left = held[hops], held[-hops]
    mine = lax.all_to_all(scaled, FS, 0, 0, tiled=True)

    dists = [0]
    for step in range(1, zs // 2 + 1):
        dists.append(step)
        if step < zs - step:
            dists.append(-step)
    cut = 2 * hops
    halves = (dists[:cut], dists[cut:])

    def swap(x):
        return shift(x, "core", 2, 1)

    def picked(arrays):
        count = len(arrays)
        return call(
            functools.partial(pick_body, cap, rows, count),
            [scal],
            arrays,
            [
                jax.ShapeDtypeStruct((count // 4 * 2 * slots, quarter), BF),
                jax.ShapeDtypeStruct((count // 4 * 2 * slots + 48 * count, quarter), BF),
                jax.ShapeDtypeStruct((count, 8, 256), F32),
                jax.ShapeDtypeStruct((count, 48, quarter), BF),
            ],
            count * 448 * 512 * 512,
        )

    picks = [picked([held[d] for d in halves[0]])]
    swaps = [swap(picks[0][1])]
    pair_rows = picks[0][0].shape[0]
    half = pair_rows + rows // 2
    top0 = jnp.concatenate([picks[0][0], swaps[0][: half - pair_rows]], axis=0)
    bot0 = jnp.concatenate([swaps[0][half - pair_rows : pair_rows], tokens], axis=0)
    at0 = shift(top0, "tp", tps, 1)
    bb0 = shift(bot0, "tp", tps, -1)
    ab0 = shift(bot0, "tp", tps, 1)
    bt0 = shift(top0, "tp", tps, -1)
    c0 = shift(at0, "tp", tps, 1)
    d0 = shift(bb0, "tp", tps, -1)
    right7 = shift(right, "z", zs, 1)
    left7 = shift(left, "z", zs, -1)
    right8 = shift(right7, "z", zs, 1)
    quads = [(top0, bot0, at0, ab0, bt0, bb0, c0, d0)]
    ring = ring_gather(mine, "grp", groups)
    placed = by_group(ring, grp, groups)
    gate_local, up_local = (
        jnp.concatenate(placed[parts * n : parts * n + parts], axis=1)
        .reshape(2 * zs, 2, 64, 128)
        .transpose(1, 0, 2, 3)
        .reshape(2, 128 * zs, 128)
        for n in range(2)
    )

    dshape = down_experts.shape
    rcut = min(parts, 2)
    ccut = parts // rcut
    dsel = lax.dynamic_index_in_dim(
        down_experts.reshape(dshape[0] // 2, 2, *dshape[1:]), grp // parts, 1, False
    ).astype(BF)
    if parts > 1:
        part = lax.rem(grp, parts)
        rsize, csize = dshape[1] // rcut, dshape[2] // ccut
        dsel = lax.dynamic_slice(
            dsel,
            (0, part // ccut * rsize, lax.rem(part, ccut) * csize),
            (dsel.shape[0], rsize, csize),
        )

    picks.append(picked([left, right7, left7, right8]))
    swaps.append(swap(picks[1][1]))
    pair_rows = picks[1][0].shape[0]
    x1 = jnp.concatenate([picks[1][0], swaps[1][:pair_rows]], axis=0)
    quads.append(quarters(x1, tps))

    dmine = lax.all_to_all(dsel, FS, 0, 0, tiled=True)
    ring = ring_gather(dmine, "grp", groups)
    placed = by_group(ring, grp, groups)
    downs = []
    for n in range(2):
        mineset = placed[parts * n : parts * n + parts]
        downs.append(
            jnp.concatenate(
                [
                    jnp.concatenate(mineset[ccut * r : ccut * r + ccut], axis=2)
                    for r in range(rcut)
                ],
                axis=1,
            )
        )

    sgate_local, sup_local, sdown_cols = call(
        functools.partial(spread_body, dists),
        [scal],
        [picks[0][3], picks[1][3], swaps[0], swaps[1]],
        [
            jax.ShapeDtypeStruct((128 * zs, 128), BF),
            jax.ShapeDtypeStruct((128 * zs, 128), BF),
            jax.ShapeDtypeStruct((32 * zs, 512), BF),
        ],
        10**6,
    )

    dense = {}
    srows = None
    for n in range(2):
        shared = n == 1
        nblock = picks[n][0].shape[0] // slots * 2
        arows = nblock * slots + (rows if shared else 0)
        extra = [sgate_local, sup_local, *quads[0]] if shared else []
        (act,) = call(
            functools.partial(
                hidden_body, slots, nblock, len(quads[n]), quarter * tps, shared
            ),
            [scal],
            [*quads[n], gate_local, up_local, *extra],
            [jax.ShapeDtypeStruct((arows, 128), BF)],
            2 * arows * 2048 * 256,
        )
        outs = [jax.ShapeDtypeStruct((nblock // 4, 2, slots, quarter), BF)] * 2
        if shared:
            outs.append(jax.ShapeDtypeStruct((rows, quarter), F32))
        acts = quarters(act, tps)
        res = call(
            functools.partial(down_body, slots, nblock, shared),
            [scal],
            [*acts, *downs, *([sdown_cols] if shared else [])],
            outs,
            2 * arows * 512 * 512,
        )
        if shared:
            srows = res[2]
        count = len(halves[n])
        blocks = call(
            functools.partial(mix_body, rows, slots),
            [],
            [res[0], swap(res[1]), picks[n][2]],
            [jax.ShapeDtypeStruct((rows, quarter), BF)] * count,
            count * 2 * 256 * 448 * 512,
        )
        dense.update(zip(halves[n], blocks))

    def inward(left, right, at):
        left = shift(left, "z", zs, -1)
        right = shift(right, "z", zs, 1)
        return left + dense[at], right + dense[1 - at]

    far = zs // 2
    left, right = inward(dense[far], dense[1 - far], far - 1)
    outgoing = jnp.stack(
        [w.reshape(4, 8 * zs, quarter) for w in (*downs, sdown_cols)], axis=1
    )
    arrived = lax.all_to_all(outgoing, "tp", 0, 0, tiled=True)
    for at in range(far - 2, 0, -1):
        left, right = inward(left, right, at)
    down_local, sdown_local = call(
        place_body,
        [],
        [arrived],
        [
            jax.ShapeDtypeStruct((2, 8 * zs, quarter * tps), BF),
            jax.ShapeDtypeStruct((8 * zs, quarter * tps), BF),
        ],
        10**6,
    )
    left = shift(left, "z", zs, -1)
    mixed = (left.astype(F32) + right.astype(F32) + srows).astype(BF)
    return (
        mixed,
        gate_local,
        up_local,
        down_local,
        sgate_local,
        sup_local,
        sdown_local,
    )


def solution(mesh):
    groups, fs, tps = (mesh.shape[a] for a in ("grp", "fs", "tp"))
    zs = fs // 2
    wide = Mesh(mesh.devices.reshape(groups, zs, 2, tps), ("grp", "z", "core", "tp"))
    fsx = ("z", "core")
    return jax.shard_map(
        functools.partial(layer, (groups, zs, tps)),
        mesh=wide,
        in_specs=(
            P(("grp", *fsx), "tp"),
            P(("grp", *fsx), None),
            P(("grp", *fsx), None),
            P(fsx),
            P(None, fsx, "tp"),
            P(None, fsx, "tp"),
            P(None, fsx, "tp"),
            P(fsx, "tp"),
            P(fsx, "tp"),
            P(fsx, "tp"),
        ),
        out_specs=(
            P(("grp", *fsx), "tp"),
            P(("grp", *fsx), None, "tp"),
            P(("grp", *fsx), None, "tp"),
            P(("grp", *fsx), "tp", None),
            P("grp", "tp"),
            P("grp", "tp"),
            P(("grp", "tp"), None),
        ),
        check_vma=False,
    )
```

```python
import functools

import jax
import jax.numpy as jnp
from jax import lax
from jax.experimental import pallas as pl
from jax.experimental.pallas import tpu as pltpu
from jax.sharding import Mesh
from jax.sharding import PartitionSpec as P


BF = jnp.bfloat16
F32 = jnp.float32
LANES = 128
VMEM = pl.BlockSpec(memory_space=pltpu.VMEM)
SMEM = pl.BlockSpec(memory_space=pltpu.SMEM)


def call(body, scalars, arrays, outs, flops):
    moved = sum(a.size * a.dtype.itemsize for a in arrays) + sum(
        o.size * o.dtype.itemsize for o in outs
    )
    return pl.pallas_call(
        body,
        out_shape=tuple(outs),
        in_specs=[SMEM] * len(scalars) + [VMEM] * len(arrays),
        out_specs=tuple([VMEM] * len(outs)),
        cost_estimate=pl.CostEstimate(flops=flops, bytes_accessed=moved, transcendentals=0),
    )(*scalars, *arrays)


def shift(x, axis, size, by):
    return lax.ppermute(x, axis, [(i, (i + by) % size) for i in range(size)])


def ring_gather(x, axis, size):
    held = {0: x}
    right = left = x
    for step in range(1, size // 2 + 1):
        right = shift(right, axis, size, 1)
        held[step] = right
        if step < size - step:
            left = shift(left, axis, size, -1)
            held[-step] = left
    return held


def quarters(x, size):
    half = x.shape[0] // 2
    a = shift(x, "tp", size, 1)
    b = shift(x, "tp", size, -1)
    c = shift(a[:half], "tp", size, 1)
    d = shift(b[half:], "tp", size, -1)
    return x, a, b, c, d


def pack_body(experts, tok, routes, weights, sgate, sup, sdown, gain, chunk, meta):
    rows = tok.shape[0]
    top = routes.shape[0]
    chunk[:rows, :] = tok[...]
    which = lax.broadcasted_iota(jnp.int32, (experts, rows), 0)
    named = [routes[k : k + 1, :] == which for k in range(top)]
    member = sum(jnp.where(n, 1.0, 0.0) for n in named)
    before = lax.broadcasted_iota(jnp.int32, (rows, rows), 0) < lax.broadcasted_iota(
        jnp.int32, (rows, rows), 1
    )
    count = jnp.dot(
        member.astype(BF), jnp.where(before, 1.0, 0.0).astype(BF), preferred_element_type=F32
    )
    ids = routes[...].astype(F32)
    w = weights[...]
    spare = rows - LANES
    meta[...] = jnp.full(meta.shape, -1.0, F32)
    for k in range(top):
        place = jnp.sum(jnp.where(named[k], count, 0.0), axis=0, keepdims=True)
        meta[16 + k : 17 + k, :] = place[:, :LANES]
        meta[24 + k : 25 + k, :spare] = place[:, LANES:]
    meta[0:top, :] = ids[:, :LANES]
    meta[8 : 8 + top, :spare] = ids[:, LANES:]
    meta[32 : 32 + top, :] = w[:, :LANES]
    meta[40 : 40 + top, :spare] = w[:, LANES:]
    scale = jnp.transpose(jnp.broadcast_to(gain[...], (8, 64)))[:, :1]
    g = (sgate[...] * scale).astype(BF)
    u = (sup[...] * scale).astype(BF)
    for n in range(2):
        at = slice(32 * n, 32 * n + 32)
        chunk[rows : rows + 32, 128 * n : 128 * n + 128] = g[at]
        chunk[rows : rows + 32, 256 + 128 * n : 384 + 128 * n] = u[at]
    chunk[rows + 32 : rows + 48, :] = sdown[...].astype(BF)
    for n in range(4):
        chunk[rows + 48 : rows + 64, 128 * n : 128 * n + 128] = meta[
            16 * n : 16 * n + 16, :
        ].astype(BF)


def pick_body(cap, rows, count, scal, *refs):
    blocks = refs[:count]
    mine, other, keys, pack = refs[count:]
    first = (scal[3], scal[4])
    slots = 4 * cap
    ngroup = len(blocks) // 4
    line = lax.broadcasted_iota(jnp.int32, (slots, 256), 0).astype(F32)
    shared_at = ngroup * 2 * slots
    for g in range(ngroup):
        sel = []
        for i in range(4):
            b = 4 * g + i
            ref = blocks[b]
            extra = ref[rows : rows + 48, :]
            pack[b] = extra
            other[shared_at + 48 * b : shared_at + 48 * b + 48, :] = extra
            meta = ref[rows + 48 : rows + 64, :].astype(F32)
            ids, pos, wts = (
                jnp.concatenate(
                    [meta[0:8, 128 * n : 128 * n + 128], meta[8:16, 128 * n : 128 * n + 128]],
                    axis=1,
                )
                for n in range(3)
            )
            col = []
            for h in range(2):
                for j in range(2):
                    hit = ids == (first[h] + j).astype(F32)
                    key = (
                        jnp.sum(jnp.where(hit, pos + (1.0 + cap * i), 0.0), axis=0, keepdims=True)
                        - 1.0
                    )
                    wt = jnp.sum(jnp.where(hit, wts, 0.0), axis=0, keepdims=True)
                    n = 2 * h + j
                    keys[b, n : n + 1, :] = key
                    keys[b, 4 + n : 5 + n, :] = wt
                    col.append(jnp.where(line == key, 1.0, 0.0).astype(BF))
            sel.append(jnp.concatenate(col, axis=0))
        x = jnp.concatenate([blocks[4 * g + i][:256, :] for i in range(4)], axis=0)
        got = jnp.dot(jnp.concatenate(sel, axis=1), x, preferred_element_type=F32).astype(BF)
        at = 2 * slots * g
        mine[at : at + 2 * slots, :] = got[: 2 * slots]
        other[at : at + 2 * slots, :] = got[2 * slots :]


def spread_body(dists, scal, own0, own1, par0, par1, gate, up, down):
    z = scal[0]
    core = scal[1]
    size = len(dists)
    count = own0.shape[0]
    for k, dist in enumerate(dists):
        at = lax.rem(z - dist + size, size) * 2
        own, par = (own0, par0) if k < count else (own1, par1)
        n = k if k < count else k - count
        base = par.shape[0] - 48 * own.shape[0] + 48 * n
        for block, who in ((own[n], core), (par[base : base + 48, :], 1 - core)):
            row = at + who
            for m in range(2):
                dst = pl.ds(pl.multiple_of(row * 64 + 32 * m, 32), 32)
                gate[dst, :] = block[0:32, 128 * m : 128 * m + 128]
                up[dst, :] = block[0:32, 256 + 128 * m : 384 + 128 * m]
            down[pl.ds(pl.multiple_of(row * 16, 16), 16), :] = block[32:48, :]


def silu_product(g, u, r):
    v = g * r
    return (v / (1.0 + jnp.exp(-v)) * (u * r)).astype(BF)


def pieces(refs):
    half = refs[-1].shape[0]

    def block(q, start, size):
        if q < 3 and len(refs) == 5:
            return refs[q][start : start + size, :]
        first = refs[-2] if q == 3 else refs[2 * q]
        second = refs[-1] if q == 3 else refs[2 * q + 1]
        if start + size <= half:
            return first[start : start + size, :]
        return second[start - half : start - half + size, :]

    return block


def turns(tp):
    return [lax.rem(tp + s, 4) for s in (0, 3, 1, 2)]


def hidden_body(slots, nblock, nx, width, shared, scal, *refs):
    gate, up = refs[nx : nx + 2]
    out = refs[-1]
    order = turns(scal[2])

    def product(take, weight):
        total = None
        square = None
        for q in range(4):
            x = take(q)
            part = jnp.dot(x, weight(order[q]), preferred_element_type=F32)
            wide = x.astype(F32)
            sq = wide * wide
            sq = sq[:, 0:128] + sq[:, 128:256] + sq[:, 256:384] + sq[:, 384:512]
            total = part if total is None else total + part
            square = sq if square is None else square + sq
        r = lax.rsqrt(jnp.sum(square, axis=1, keepdims=True) * (1.0 / width) + 1e-06)
        return silu_product(total[:, :128], total[:, 128:], r)

    block = pieces(refs[:nx])
    for e in range(2):
        act = product(
            lambda q: jnp.concatenate(
                [block(q, slots * r, slots) for r in range(e, nblock, 2)], axis=0
            ),
            lambda q: jnp.concatenate(
                [w[pl.ds(q * 8, 8), e].reshape(512, 128) for w in (gate, up)], axis=1
            ),
        )
        for n in range(nblock // 2):
            r = 2 * n + e
            out[slots * r : slots * r + slots, :] = act[slots * n : slots * n + slots]
    if shared:
        sgate, sup = refs[nx + 2 : nx + 4]
        base = nblock * slots
        wide_block = pieces(refs[nx + 4 : -1])
        at0 = 2 * refs[-2].shape[0] - 2 * slots
        out[base : base + 2 * slots, :] = product(
            lambda q: wide_block(q, at0, 2 * slots),
            lambda q: jnp.concatenate(
                [w[pl.ds(pl.multiple_of(q * 512, 512), 512), :] for w in (sgate, sup)], axis=1
            ),
        )


def down_body(slots, nblock, shared, scal, *refs):
    downs = refs[5:7]
    block = pieces(refs[:5])
    near, far = refs[8:10] if shared else refs[7:9]
    order = turns(scal[2])
    for e in range(2):
        total = None
        for q in range(4):
            x = jnp.concatenate(
                [block(q, slots * r, slots) for r in range(e, nblock, 2)], axis=0
            )
            w = downs[e][pl.ds(order[q] * 8, 8)].reshape(128, 512)
            part = jnp.dot(x, w, preferred_element_type=F32)
            total = part if total is None else total + part
        rows = total.astype(BF)
        count = nblock // 4
        for n in range(2 * count):
            (near if n < count else far)[n % count, e] = rows[slots * n : slots * n + slots]
    if shared:
        sdown, srows = refs[7], refs[10]
        base = nblock * slots
        total = None
        for q in range(4):
            x = block(q, base, 2 * slots)
            w = sdown[pl.ds(pl.multiple_of(order[q] * 128, 128), 128), :]
            part = jnp.dot(x, w, preferred_element_type=F32)
            total = part if total is None else total + part
        srows[...] = total


def mix_body(rows, slots, near, far, keys, *outs):
    line = lax.broadcasted_iota(jnp.int32, (slots, 256), 0).astype(F32)
    for g in range(near.shape[0]):
        held = jnp.concatenate([near[g, 0], near[g, 1], far[g, 0], far[g, 1]], axis=0)
        for i in range(4):
            b = 4 * g + i
            spread = jnp.concatenate(
                [
                    jnp.where(line == keys[b, n : n + 1, :], keys[b, 4 + n : 5 + n, :], 0.0)
                    for n in range(4)
                ],
                axis=0,
            ).astype(BF)
            dense = lax.dot_general(
                spread, held, (((0,), (0,)), ((), ())), preferred_element_type=F32
            )
            outs[b][...] = dense[:rows].astype(BF)


def place_body(blocks, routed, common):
    width = blocks.shape[3]
    for q in range(blocks.shape[0]):
        at = slice(width * q, width * q + width)
        for n in range(2):
            routed[n, :, at] = blocks[q, n]
        common[:, at] = blocks[q, 2]


def by_group(ring, grp, groups):
    if groups == 2:
        return [jnp.where(grp == g, ring[0], ring[1]) for g in range(2)]
    stack = jnp.stack([ring[k if k <= groups // 2 else k - groups] for k in range(groups)])
    return [
        lax.dynamic_index_in_dim(stack, lax.rem(grp - g + groups, groups), 0, False)
        for g in range(groups)
    ]


def layer(
    sizes,
    tokens,
    routes,
    route_weights,
    norm_gain,
    gate_experts,
    up_experts,
    down_experts,
    shared_gate,
    shared_up,
    shared_down,
):
    groups, zs, tps = sizes
    rows, quarter = tokens.shape
    top = routes.shape[1]
    experts = gate_experts.shape[0]
    cap = 4 * rows * top // (3 * experts)
    slots = 4 * cap
    z = lax.axis_index("z")
    core = lax.axis_index("core")
    tp = lax.axis_index("tp")
    fs = 2 * z + core
    scal = jnp.stack([z, core, tp, 2 * fs, 2 * (2 * z + 1 - core), z, z, z]).astype(jnp.int32)
    FS = ("z", "core")
    grp = lax.axis_index("grp")
    tie = lax.optimization_barrier

    (chunk,) = pl.pallas_call(
        functools.partial(pack_body, experts),
        name="pack",
        out_shape=(jax.ShapeDtypeStruct((rows + 64, quarter), BF),),
        in_specs=[VMEM] * 7,
        out_specs=(VMEM,),
        scratch_shapes=[pltpu.VMEM((64, LANES), F32)],
        cost_estimate=pl.CostEstimate(flops=10**7, bytes_accessed=10**6, transcendentals=0),
    )(
        tokens,
        routes.T,
        route_weights.T,
        shared_gate,
        shared_up,
        shared_down,
        norm_gain[None, :],
    )
    hops = zs // 2 - 2
    held = {0: chunk}
    right = left = chunk
    for step in range(1, hops + 1):
        held[step] = right = shift(right, "z", zs, 1)
        held[-step] = left = shift(left, "z", zs, -1)

    parts = groups // 2
    share = gate_experts.shape[1] // parts
    scaled = (
        jnp.where(grp < parts, gate_experts, up_experts) * norm_gain[None, :, None]
    ).astype(BF)
    if parts > 1:
        scaled = lax.dynamic_slice_in_dim(scaled, lax.rem(grp, parts) * share, share, 1)
    scaled, right, left = tie((scaled, right, left))
    held[hops], held[-hops] = right, left
    mine = lax.all_to_all(scaled, FS, 0, 0, tiled=True)

    dists = [0]
    for step in range(1, zs // 2 + 1):
        dists.append(step)
        if step < zs - step:
            dists.append(-step)
    cut = 2 * hops
    halves = (dists[:cut], dists[cut:])

    def swap(x):
        return shift(x, "core", 2, 1)

    def picked(arrays):
        count = len(arrays)
        return call(
            functools.partial(pick_body, cap, rows, count),
            [scal],
            arrays,
            [
                jax.ShapeDtypeStruct((count // 4 * 2 * slots, quarter), BF),
                jax.ShapeDtypeStruct((count // 4 * 2 * slots + 48 * count, quarter), BF),
                jax.ShapeDtypeStruct((count, 8, 256), F32),
                jax.ShapeDtypeStruct((count, 48, quarter), BF),
            ],
            count * 448 * 512 * 512,
        )

    picks = [picked([held[d] for d in halves[0]])]
    swaps = [swap(picks[0][1])]
    pair_rows = picks[0][0].shape[0]
    half = pair_rows + rows // 2
    top0 = jnp.concatenate([picks[0][0], swaps[0][: half - pair_rows]], axis=0)
    bot0 = jnp.concatenate([swaps[0][half - pair_rows : pair_rows], tokens], axis=0)
    at0 = shift(top0, "tp", tps, 1)
    bb0 = shift(bot0, "tp", tps, -1)
    ab0 = shift(bot0, "tp", tps, 1)
    bt0 = shift(top0, "tp", tps, -1)
    c0 = shift(at0, "tp", tps, 1)
    d0 = shift(bb0, "tp", tps, -1)
    right7 = shift(right, "z", zs, 1)
    left7 = shift(left, "z", zs, -1)
    right8 = shift(right7, "z", zs, 1)
    quads = [(top0, bot0, at0, ab0, bt0, bb0, c0, d0)]
    ring = ring_gather(mine, "grp", groups)
    placed = by_group(ring, grp, groups)
    arrived_pair = [
        jnp.concatenate(placed[parts * n : parts * n + parts], axis=1).reshape(2 * zs, 2, 64, 128)
        for n in range(2)
    ]
    gate_local, up_local = (
        w.transpose(1, 0, 2, 3).reshape(2, 128 * zs, 128) for w in arrived_pair
    )

    dshape = down_experts.shape
    rcut = min(parts, 2)
    ccut = parts // rcut
    dsel = lax.dynamic_index_in_dim(
        down_experts.reshape(dshape[0] // 2, 2, *dshape[1:]), grp // parts, 1, False
    ).astype(BF)
    if parts > 1:
        part = lax.rem(grp, parts)
        rsize, csize = dshape[1] // rcut, dshape[2] // ccut
        dsel = lax.dynamic_slice(
            dsel,
            (0, part // ccut * rsize, lax.rem(part, ccut) * csize),
            (dsel.shape[0], rsize, csize),
        )

    picks.append(picked([left, right7, left7, right8]))
    swaps.append(swap(picks[1][1]))
    pair_rows = picks[1][0].shape[0]
    x1 = jnp.concatenate([picks[1][0], swaps[1][:pair_rows]], axis=0)
    quads.append(quarters(x1, tps))

    dmine = lax.all_to_all(dsel, FS, 0, 0, tiled=True)
    ring = ring_gather(dmine, "grp", groups)
    placed = by_group(ring, grp, groups)
    downs = []
    for n in range(2):
        mineset = placed[parts * n : parts * n + parts]
        downs.append(
            jnp.concatenate(
                [
                    jnp.concatenate(mineset[ccut * r : ccut * r + ccut], axis=2)
                    for r in range(rcut)
                ],
                axis=1,
            )
        )

    sgate_local, sup_local, sdown_cols = call(
        functools.partial(spread_body, dists),
        [scal],
        [picks[0][3], picks[1][3], swaps[0], swaps[1]],
        [
            jax.ShapeDtypeStruct((128 * zs, 128), BF),
            jax.ShapeDtypeStruct((128 * zs, 128), BF),
            jax.ShapeDtypeStruct((32 * zs, 512), BF),
        ],
        10**6,
    )

    dense = {}
    srows = None
    for n in range(2):
        shared = n == 1
        nblock = picks[n][0].shape[0] // slots * 2
        arows = nblock * slots + (rows if shared else 0)
        extra = [sgate_local, sup_local, *quads[0]] if shared else []
        (act,) = call(
            functools.partial(
                hidden_body, slots, nblock, len(quads[n]), quarter * tps, shared
            ),
            [scal],
            [*quads[n], *arrived_pair, *extra],
            [jax.ShapeDtypeStruct((arows, 128), BF)],
            2 * arows * 2048 * 256,
        )
        outs = [jax.ShapeDtypeStruct((nblock // 4, 2, slots, quarter), BF)] * 2
        if shared:
            outs.append(jax.ShapeDtypeStruct((rows, quarter), F32))
        acts = quarters(act, tps)
        res = call(
            functools.partial(down_body, slots, nblock, shared),
            [scal],
            [*acts, *downs, *([sdown_cols] if shared else [])],
            outs,
            2 * arows * 512 * 512,
        )
        if shared:
            srows = res[2]
        count = len(halves[n])
        blocks = call(
            functools.partial(mix_body, rows, slots),
            [],
            [res[0], swap(res[1]), picks[n][2]],
            [jax.ShapeDtypeStruct((rows, quarter), BF)] * count,
            count * 2 * 256 * 448 * 512,
        )
        dense.update(zip(halves[n], blocks))

    def inward(left, right, at):
        left = shift(left, "z", zs, -1)
        right = shift(right, "z", zs, 1)
        return left + dense[at], right + dense[1 - at]

    far = zs // 2
    left, right = inward(dense[far], dense[1 - far], far - 1)
    outgoing = jnp.stack(
        [w.reshape(4, 8 * zs, quarter) for w in (*downs, sdown_cols)], axis=1
    )
    arrived = lax.all_to_all(outgoing, "tp", 0, 0, tiled=True)
    for at in range(far - 2, 0, -1):
        left, right = inward(left, right, at)
    down_local, sdown_local = call(
        place_body,
        [],
        [arrived],
        [
            jax.ShapeDtypeStruct((2, 8 * zs, quarter * tps), BF),
            jax.ShapeDtypeStruct((8 * zs, quarter * tps), BF),
        ],
        10**6,
    )
    left = shift(left, "z", zs, -1)
    mixed = (left.astype(F32) + right.astype(F32) + srows).astype(BF)
    return (
        mixed,
        gate_local,
        up_local,
        down_local,
        sgate_local,
        sup_local,
        sdown_local,
    )


def solution(mesh):
    groups, fs, tps = (mesh.shape[a] for a in ("grp", "fs", "tp"))
    zs = fs // 2
    wide = Mesh(mesh.devices.reshape(groups, zs, 2, tps), ("grp", "z", "core", "tp"))
    fsx = ("z", "core")
    return jax.shard_map(
        functools.partial(layer, (groups, zs, tps)),
        mesh=wide,
        in_specs=(
            P(("grp", *fsx), "tp"),
            P(("grp", *fsx), None),
            P(("grp", *fsx), None),
            P(fsx),
            P(None, fsx, "tp"),
            P(None, fsx, "tp"),
            P(None, fsx, "tp"),
            P(fsx, "tp"),
            P(fsx, "tp"),
            P(fsx, "tp"),
        ),
        out_specs=(
            P(("grp", *fsx), "tp"),
            P(("grp", *fsx), None, "tp"),
            P(("grp", *fsx), None, "tp"),
            P(("grp", *fsx), "tp", None),
            P("grp", "tp"),
            P("grp", "tp"),
            P(("grp", "tp"), None),
        ),
        check_vma=False,
    )
```
